256 devices in a mesh: rep: 2 (over z_hi), fs: 16 (over z_lo, x), tp: 8 (over y, core).
Axes of the slice: x: 4, y: 4, z: 8 (z_hi: 2, z_lo: 4; z = z_hi * 4 + z_lo), core: 2. Of those that a mesh axis runs over, the one named last changes fastest.
Arguments:
- tokens: bfloat16 [32768, 2048], P(('rep', 'fs'), 'tp'), may hold values from -6 to 6
- mix_gain: float32 [2048], replicated, may hold values from 0.1 to 1.9
- query_weight: bfloat16 [2048, 512], P('fs', 'tp'), may hold values from -0.125 to 0.125
- key_weight: bfloat16 [2048, 512], P('fs', 'tp'), may hold values from -0.125 to 0.125
- value_weight: bfloat16 [2048, 1024], P('fs', 'tp'), may hold values from -0.125 to 0.125
- gate_weight: bfloat16 [2048, 1024], P('fs', 'tp'), may hold values from -0.125 to 0.125
- out_weight: bfloat16 [1024, 2048], P('tp', 'fs'), may hold values from -0.1875 to 0.1875
- head_gain: float32 [8, 128], P('tp'), may hold values from 0.1 to 1.9
- ffn_gain: float32 [2048], replicated, may hold values from 0.1 to 1.9
- ffn_gate: bfloat16 [2048, 5632], P('fs', 'tp'), may hold values from -0.125 to 0.125
- ffn_up: bfloat16 [2048, 5632], P('fs', 'tp'), may hold values from -0.125 to 0.125
- ffn_down: bfloat16 [5632, 2048], P('tp', 'fs'), may hold values from -0.078125 to 0.078125
Outputs:
- layer_out: bfloat16 [32768, 2048], P(('rep', 'fs'), 'tp')
The draws below stay inside these ranges and needn't reach their ends.
All inputs are finite; a program needn't handle non-finite values.
Results may differ from the reference program's by a relative error of at most 0.03.
Values may be sent and summed in bfloat16 or wider, within the bound.
A program may use at most 128 MiB of HBM per device.

```python
import jax
import jax.numpy as jnp
from jax import lax

D = 2048
HEADS = 8
DK = 64
DV = 128
FF = 5632
SEQ = 256
TOKENS = 32768
N_TP = 8


def levels(rng, extent, shards, least, largest):
    gain = 1.0
    for dim, parts in shards:
        steps = jax.random.uniform(jax.random.fold_in(jax.random.fold_in(rng, 6), dim), (parts,), jnp.float32, least / len(shards), largest / len(shards))
        gain = gain * jnp.repeat(jnp.exp(steps), extent[dim] // parts).reshape((-1,) + (1,) * (len(extent) - 1 - dim))
    return gain


def normal_values(key, extent, scale, most, shards=(), held_as=jnp.bfloat16):
    level = levels(key, extent, shards, -0.22, 0.18) if shards else 1.0
    values = jax.random.normal(key, extent, jnp.float32) * scale * level
    return jnp.minimum(jnp.maximum(values, -most), most).astype(held_as)


def setup_inputs(seed: int = 0) -> dict:
    seeds = jax.random.split(jax.random.key(seed), 13)
    return {
        "tokens": normal_values(seeds[0], (TOKENS, D), 1.0, 6.0, ((0, 32), (1, 8))),
        "mix_gain": jnp.clip(1.0 + 0.18 * jax.random.normal(seeds[1], (D,), jnp.float32), 0.1, 1.9),
        "query_weight": normal_values(seeds[2], (D, HEADS * DK), D ** -0.5, 0.125, ((0, 16), (1, 8))),
        "key_weight": normal_values(seeds[3], (D, HEADS * DK), D ** -0.5, 0.125, ((0, 16), (1, 8))),
        "value_weight": normal_values(seeds[4], (D, HEADS * DV), D ** -0.5, 0.125, ((0, 16), (1, 8))),
        "gate_weight": normal_values(seeds[5], (D, HEADS * DV), D ** -0.5, 0.125, ((0, 16), (1, 8))),
        "out_weight": normal_values(seeds[6], (HEADS * DV, D), (HEADS * DV) ** -0.5, 0.1875, ((0, 8), (1, 16))),
        "head_gain": jnp.clip(1.0 + 0.18 * jax.random.normal(seeds[7], (HEADS, DV), jnp.float32), 0.1, 1.9),
        "ffn_gain": jnp.clip(1.0 + 0.18 * jax.random.normal(seeds[8], (D,), jnp.float32), 0.1, 1.9),
        "ffn_gate": normal_values(seeds[9], (D, FF), D ** -0.5, 0.125, ((0, 16), (1, 8))),
        "ffn_up": normal_values(seeds[10], (D, FF), D ** -0.5, 0.125, ((0, 16), (1, 8))),
        "ffn_down": normal_values(seeds[11], (FF, D), FF ** -0.5, 0.078125, ((0, 8), (1, 16))),
    }


epsilon = 1e-06
rope_base = 10000.0

def norm_rows(values, gain_row):
    floats = values.astype(jnp.float32)
    scaled = floats * lax.rsqrt(lax.optimization_barrier(jnp.mean(floats * floats, axis=-1, keepdims=True)) + epsilon)
    return (scaled * gain_row).astype(jnp.bfloat16)

def rotate(values, positions):
    half_dim = values.shape[-1] // 2
    frequency = rope_base ** (-jnp.linspace(0.0, 1.0, half_dim, dtype=jnp.float32))
    angles = positions.astype(jnp.float32)[:, None] * frequency[None, :]
    cosine = jnp.cos(angles)[:, None, :]
    sine_part = jnp.sin(angles)[:, None, :]
    paired = values.reshape(values.shape[:-1] + (half_dim, 2))
    leading = paired[..., 0]
    trailing = paired[..., 1]
    turned = jnp.stack([leading * cosine - trailing * sine_part, leading * sine_part + trailing * cosine], axis=-1)
    return turned.reshape(values.shape)

def log_decay(head_index, total_heads):
    return jnp.log1p(-jnp.exp2(-5.0 - 4.0 * head_index.astype(jnp.float32) / (total_heads - 1)))

def split_sum(left, right):
    columns = left.shape[1] // N_TP
    summed = jnp.zeros((left.shape[0], right.shape[1]), jnp.float32)
    for segment in range(N_TP):
        partial_value = jnp.dot(left[:, segment * columns:(segment + 1) * columns], right[segment * columns:(segment + 1) * columns], preferred_element_type=jnp.float32).astype(jnp.bfloat16)
        summed = summed + lax.optimization_barrier(partial_value).astype(jnp.float32)
    return summed

def reference(tokens, mix_gain, query_weight, key_weight, value_weight, gate_weight, out_weight, head_gain, ffn_gain, ffn_gate, ffn_up, ffn_down):
    highest = lax.Precision.HIGHEST
    row_count = tokens.shape[0]
    normed = norm_rows(tokens, mix_gain)

    def project(weight):
        return jnp.dot(normed, weight, preferred_element_type=jnp.float32).astype(jnp.bfloat16)
    positions = jnp.arange(row_count, dtype=jnp.int32) % SEQ
    queries = rotate(project(query_weight).astype(jnp.float32).reshape(row_count, HEADS, DK), positions)
    key_rows = rotate(project(key_weight).astype(jnp.float32).reshape(row_count, HEADS, DK), positions) * DK ** (-0.5)
    value_rows = project(value_weight).astype(jnp.float32).reshape(row_count, HEADS, DV)
    gate_rows = project(gate_weight).astype(jnp.float32)
    decay_rates = log_decay(jnp.arange(HEADS, dtype=jnp.int32), HEADS)
    offsets = jnp.arange(SEQ, dtype=jnp.int32)
    distance = (offsets[:, None] - offsets[None, :]).astype(jnp.float32)
    decay_mask = jnp.where(distance[None] >= 0.0, jnp.exp(jnp.maximum(distance, 0.0)[None] * decay_rates[:, None, None]), 0.0)
    seq_count = row_count // SEQ

    def one_sequence(inputs):
        query_seq, key_seq, value_seq = inputs
        scores = jnp.einsum('ihd,jhd->hij', query_seq, key_seq, precision=highest) * decay_mask
        return jnp.einsum('hij,jhv->ihv', scores, value_seq, precision=highest)
    retained = lax.map(one_sequence, (queries.reshape(seq_count, SEQ, HEADS, DK), key_rows.reshape(seq_count, SEQ, HEADS, DK), value_rows.reshape(seq_count, SEQ, HEADS, DV)))
    retained = retained.reshape(row_count, HEADS, DV)
    center = lax.optimization_barrier(jnp.mean(retained, axis=-1, keepdims=True))
    spread = lax.optimization_barrier(jnp.mean(jnp.square(retained - center), axis=-1, keepdims=True))
    grouped = (retained - center) * lax.rsqrt(spread + epsilon) * head_gain[None]
    mixed = (grouped.reshape(row_count, HEADS * DV) * jax.nn.silu(gate_rows)).astype(jnp.bfloat16)
    residual = (tokens.astype(jnp.float32) + split_sum(mixed, out_weight)).astype(jnp.bfloat16)
    normed_ffn = norm_rows(residual, ffn_gain)
    gate_hidden = jnp.dot(normed_ffn, ffn_gate, preferred_element_type=jnp.float32)
    up_hidden = jnp.dot(normed_ffn, ffn_up, preferred_element_type=jnp.float32)
    hidden = (jax.nn.silu(gate_hidden) * up_hidden).astype(jnp.bfloat16)
    return (residual.astype(jnp.float32) + split_sum(hidden, ffn_down)).astype(jnp.bfloat16)
```

```python
import functools

import jax
import jax.numpy as jnp
import numpy as np
from jax import lax
from jax.experimental import pallas as pl
from jax.experimental.pallas import tpu as pltpu
from jax.sharding import PartitionSpec as P

HEADS = 8
DK = 64
DV = 128
SEQ = 256
EPS = 1e-06
ROPE_BASE = 10000.0
F32 = jnp.float32
BF16 = jnp.bfloat16
MESH = pl.DeviceIdType.MESH
MAX_COPIES = 352

UNITS = {
    "QO": (0, 64, 32, 64, 32),
    "G0": (0, 32, 16, 32, 16),
    "G1": (64, 32, 16, 32, 16),
    "D0": (0, 176, 96, 176, 96),
    "D1": (352, 176, 96, 176, 96),
}

SCHEDULE = (
    "oz.QO", "ox.QO", "Tp.0", "stage_gu.0", "Tp.3", "g0z.QO", "ox.G0", "oz.G1",
    "g0x.QO", "fzp.QO", "fzm.QO", "fxp.QO", "fxm.QO", "Tp.2", "g1z.QO", "g2z.QO",
    "g2x.QO", "Tfa.0", "Tfb.0", "h0zp.QO", "g1x.QO", "h0xm.QO", "h0xp.QO", "h0zm.QO",
    "g3x.QO", "g3z.QO", "Tfb.3", "Tfa.3", "ox.G1", "oz.G0", "h2xm.QO", "Tp.1",
    "stage_c.0", "h1xp.QO", "h2xp.QO", "h1xm.QO", "h1zm.QO", "Tfb.2", "h1zp.QO", "h2zp.QO",
    "Tg.0", "h2zm.QO", "h3xp.QO", "h3xm.QO", "h3zp.QO", "h3zm.QO", "g0z.G0", "g0x.G0",
    "Tfa.2", "Tg.3", "Td.0", "fzm.G1", "norm1.0", "fzp.G1", "fzm.G0", "fxp.G0",
    "fzp.G0", "g1x.G0", "g1z.G0", "fxm.G0", "Td.3", "g2x.G0", "fxm.G1", "g0x.G1",
    "g2z.G0", "norm1.3", "stage_d.0", "oz.D0", "Tfa.1", "Tfb.1", "ox.D1", "oz.D1",
    "e.QO", "mixa.3", "Tg.2", "mixb.3", "Rx.3", "mixa.0", "mixb.0", "Rx.0",
    "Ra.3", "Td.2", "g3z.G0", "h0zp.G0", "g3x.G0", "fxp.G1", "g2z.G1", "h1zm.G0",
    "h0xp.G0", "h1xp.G0", "h0xm.G0", "Tg.1", "h0zm.G0", "h2xm.G0", "h1xm.G0", "h1zp.G0",
    "norm1.2", "Ra.0", "Td.1", "mixa.2", "mixb.2", "Rba.3", "h2xp.G0", "Rbb.3",
    "h2zp.G0", "h2zm.G0", "Rx.2", "h3zm.G0", "h3xp.G0", "h3zp.G0", "h3xm.G0", "g1x.G1",
    "fxm.D1", "g3z.G1", "Rbb.0", "Rba.0", "ox.D0", "Ra.2", "g3x.G1", "g1z.G1",
    "norm1.1", "g0z.G1", "g0z.D1", "fzm.D1", "Rc.3", "g0z.D0", "fzp.D0", "Up.3",
    "fzp.D1", "fxp.D1", "g2x.G1", "e.G0", "Rc.0", "g2x.D1", "Up.0", "h1xm.G1",
    "mixa.1", "fxp.D0", "fzm.D0", "g2x.D0", "h0xp.G1", "g3z.D1", "mixb.1", "h0zm.G1",
    "Ufb.3", "g0x.D1", "Ufa.3", "h2xp.G1", "Rx.1", "h3zm.G1", "Rbb.2", "h1xp.G1",
    "fxm.D0", "h3xp.G1", "h2zp.G1", "h1zm.G1", "h1zp.G1", "h3xm.G1", "h2xm.G1", "h0zp.G1",
    "Rba.2", "Ufa.0", "Ufb.0", "h3zp.G1", "h0xm.G1", "g1x.D1", "g1x.D0", "h2zm.G1",
    "g2z.D0", "g2z.D1", "h0zm.D0", "g3x.D1", "g0x.D0", "h2xm.D0", "g3x.D0", "g1z.D0",
    "Ra.1", "h0xm.D1", "g1z.D1", "Ug.3", "g3z.D0", "h2xm.D1", "h0zp.D1", "h0zm.D1",
    "h2xp.D1", "h2xp.D0", "h3zp.D1", "Rc.2", "h3zm.D1", "h0xp.D1", "h0zp.D0", "Up.2",
    "Ud.3", "norm2.3", "Ug.0", "e.G1", "gua.3", "Rba.1", "Rbb.1", "h2zp.D1",
    "h2zm.D1", "h2zp.D0", "h1xp.D0", "h1xm.D1", "h1xm.D0", "Ud.0", "norm2.0", "h1zp.D0",
    "h3xp.D1", "h2zm.D0", "h1zm.D0", "h1xp.D1", "h3xm.D1", "gua.0", "h1zp.D1", "h3xp.D0",
    "h1zm.D1", "h0xp.D0", "h0xm.D0", "h3zp.D0", "h3zm.D0", "h3xm.D0", "Ufa.2", "Ufb.2",
    "gub.3", "Rc.1", "Up.1", "gub.0", "e.D1", "e.D0", "downa.0", "Ug.2",
    "downb.0", "downa.3", "Ud.2", "norm2.2", "Ufa.1", "Ufb.1", "Vx.0", "downb.3",
    "Vx.3", "gua.2", "gub.2", "Va.0", "Va.3", "Ug.1", "downa.2", "downb.2",
    "Ud.1", "norm2.1", "Vx.2", "gua.1", "Vba.0", "Vbb.0", "gub.1", "Va.2",
    "downa.1", "downb.1", "Vx.1", "Vba.3", "Vbb.3", "Vc.0", "Va.1", "Vba.2",
    "Vbb.2", "Vc.3", "Vba.1", "Vbb.1", "Vc.2", "Vc.1",
)


def rope_tables():
    half = DK // 2
    frequency = ROPE_BASE ** (-np.linspace(0.0, 1.0, half))
    angles = np.arange(SEQ)[:, None] * frequency[None, :]
    cosine = np.repeat(np.cos(angles), 2, axis=1)
    sine = np.repeat(np.sin(angles), 2, axis=1) * np.tile([-1.0, 1.0], half)
    scale = DK**-0.5
    return (
        np.concatenate([cosine, cosine * scale], axis=1).astype(np.float32),
        np.concatenate([sine, sine * scale], axis=1).astype(np.float32),
    )


def decay_table():
    rates = np.log1p(-np.exp2(-5.0 - 4.0 * np.arange(HEADS) / (HEADS - 1)))
    return np.broadcast_to(rates[:, None, None], (HEADS, 8, 128)).astype(np.float32)


def silu(values):
    return values / (1.0 + jnp.exp(-values))


def dot(left, right):
    return jnp.dot(left, right, preferred_element_type=F32)


def layer_kernel(
    tok_hbm,
    mix_gain_hbm,
    query_hbm,
    key_hbm,
    value_hbm,
    gate_hbm,
    out_w_hbm,
    head_gain_hbm,
    ffn_gain_hbm,
    ffn_gate_hbm,
    ffn_up_hbm,
    down_hbm,
    cos_hbm,
    sin_hbm,
    rate_hbm,
    out_hbm,
    tok,
    resid,
    normed,
    w_qo,
    w_gu,
    w_d,
    turn_qk,
    turn_gu,
    mix_gain,
    ffn_gain,
    head_gain,
    cos_ref,
    sin_ref,
    rate_ref,
    out_ref,
    mask,
    mixed,
    hidden,
    part1,
    pair1,
    sums1,
    fromp1,
    fromm1,
    relayp1,
    relaym1,
    part2,
    pair2,
    sums2,
    fromp2,
    fromm2,
    relayp2,
    relaym2,
    local_sem,
    send_sem,
    recv_sem,
):
    rep, fs, tp = lax.axis_index("rep"), lax.axis_index("fs"), lax.axis_index("tp")
    y, c = lax.div(tp, 2), lax.rem(tp, 2)
    z, x = lax.div(fs, 4), lax.rem(fs, 4)
    oc = 1 - c

    def step(value, by, size):
        return lax.rem(value + by, size)

    yp, y2, ym = step(y, 1, 4), step(y, 2, 4), step(y, 3, 4)
    xp, x2, xm = step(x, 1, 4), step(x, 2, 4), step(x, 3, 4)
    zp, z2, zm = step(z, 1, 4), step(z, 2, 4), step(z, 3, 4)
    zall = rep * 4 + z

    def z_device(place):
        return (lax.div(place, 4), lax.rem(place, 4) * 4 + x, tp)

    to_yp, to_ym = (rep, fs, yp * 2 + c), (rep, fs, ym * 2 + c)
    to_pt = (rep, fs, y * 2 + oc)
    to_xp, to_xm = (rep, z * 4 + xp, tp), (rep, z * 4 + xm, tp)
    to_zp, to_zm = z_device(step(zall, 1, 8)), z_device(step(zall, 7, 8))

    barrier = pltpu.get_barrier_semaphore()
    peers = (to_yp, to_ym, to_pt, to_xp, to_xm, to_zp, to_zm)
    for peer in peers:
        pl.semaphore_signal(barrier, inc=1, device_id=peer, device_id_type=MESH)

    ids = {}
    sent = []

    def send(key, src, dst, device):
        assert key not in ids
        k = ids[key] = len(ids)
        copy = pltpu.make_async_remote_copy(
            src_ref=src,
            dst_ref=dst,
            send_sem=send_sem.at[k],
            recv_sem=recv_sem.at[k],
            device_id=device,
            device_id_type=MESH,
        )
        copy.start()
        sent.append(copy)

    def recv(key, dst):
        k = ids[key]
        pltpu.make_async_remote_copy(
            src_ref=dst,
            dst_ref=dst,
            send_sem=send_sem.at[k],
            recv_sem=recv_sem.at[k],
            device_id=to_pt,
            device_id_type=MESH,
        ).wait_recv()

    count = [0]

    def local(src, dst):
        copy = pltpu.make_async_copy(src, dst, local_sem.at[count[0]])
        count[0] += 1
        copy.start()
        return copy

    loads = {}
    loads["qk"] = [
        local(query_hbm, turn_qk.at[pl.ds(0, DK)]),
        local(key_hbm, turn_qk.at[pl.ds(DK, DK)]),
    ]
    loads["vgo"] = [
        local(value_hbm, w_qo.at[z, x, :, pl.ds(128, 128)]),
        local(gate_hbm, w_qo.at[z, x, :, pl.ds(256, 128)]),
        local(out_w_hbm, w_qo.at[z, x, :, pl.ds(384, 128)]),
    ]
    loads["tok"] = [local(tok_hbm, tok.at[y, c])]
    loads["gu"] = []
    for j in range(6):
        width = 128 if j < 5 else 64
        for k, source in enumerate((ffn_gate_hbm, ffn_up_hbm)):
            place = pl.ds(256 * j + width * k, width)
            loads["gu"].append(local(source.at[pl.ds(128 * j, width)], turn_gu.at[place]))
    loads["down"] = [local(down_hbm, w_d.at[z, x])]
    loads["rest"] = [
        local(mix_gain_hbm, mix_gain),
        local(ffn_gain_hbm, ffn_gain),
        local(head_gain_hbm, head_gain),
        local(cos_hbm, cos_ref),
        local(sin_hbm, sin_ref),
        local(rate_hbm, rate_ref),
    ]

    def loaded(name):
        for copy in loads[name]:
            copy.wait()

    loaded("qk")
    w_qo[z, x, :, 0:128] = turn_qk[...].T
    loaded("vgo")
    loaded("tok")
    pl.semaphore_wait(barrier, len(peers))

    def stage_gate_up(_):
        loaded("gu")
        for j in range(11):
            lanes = slice(128 * j, 128 * j + 128)
            w_gu[z, x, :, lanes] = turn_gu[lanes, :].T

    def stage_down(_):
        loaded("down")

    def stage_rest(_):
        loaded("rest")
        gap = lax.broadcasted_iota(jnp.int32, (SEQ, 128), 0) - lax.broadcasted_iota(
            jnp.int32, (SEQ, 128), 1
        )
        rate = rate_ref[tp][:1, :]
        for half in range(2):
            distance = (gap - 128 * half).astype(F32)
            mask[:, 128 * half : 128 * half + 128] = jnp.where(
                distance >= 0.0, jnp.exp(jnp.maximum(distance, 0.0) * rate), 0.0
            )

    def rows_of(ch):
        return pl.ds(SEQ * ch, SEQ), pl.ds(SEQ * ch, 128), pl.ds(SEQ * ch + 128, 128)

    def gather_own(buf, tag, ch):
        rows, _, _ = rows_of(ch)
        own = buf.at[y, c, rows]
        send((tag, "yp", ch), own, own, to_yp)
        send((tag, "ym", ch), own, own, to_ym)
        send((tag, "pt0", ch), own, own, to_pt)

    def gather_forward(buf, tag, ch, side):
        rows, low, high = rows_of(ch)
        if side == "a":
            recv((tag, "yp", ch), buf.at[ym, c, rows])
            send((tag, "fp", ch), buf.at[ym, c, low], buf.at[ym, c, low], to_yp)
            send((tag, "pt1", ch), buf.at[ym, c, rows], buf.at[ym, c, rows], to_pt)
        else:
            recv((tag, "ym", ch), buf.at[yp, c, rows])
            send((tag, "fm", ch), buf.at[yp, c, high], buf.at[yp, c, high], to_ym)
            send((tag, "pt2", ch), buf.at[yp, c, rows], buf.at[yp, c, rows], to_pt)

    def gather_far(buf, tag, ch):
        rows, low, high = rows_of(ch)
        recv((tag, "fp", ch), buf.at[y2, c, low])
        recv((tag, "fm", ch), buf.at[y2, c, high])
        send((tag, "pt3", ch), buf.at[y2, c, rows], buf.at[y2, c, rows], to_pt)

    def gather_done(buf, tag, ch):
        rows, _, _ = rows_of(ch)
        recv((tag, "pt0", ch), buf.at[y, oc, rows])
        recv((tag, "pt1", ch), buf.at[ym, oc, rows])
        recv((tag, "pt2", ch), buf.at[yp, oc, rows])
        recv((tag, "pt3", ch), buf.at[y2, oc, rows])

    weight = {"QO": w_qo, "G0": w_gu, "G1": w_gu, "D0": w_d, "D1": w_d}

    def spans(unit):
        first, a, a0, b, b0 = UNITS[unit]
        return (
            pl.ds(first, a),
            pl.ds(first, a0),
            pl.ds(first + a0, a - a0),
            pl.ds(first + a, b),
            pl.ds(first + a, b0),
            pl.ds(first + a + b0, b - b0),
        )

    def near_own(unit, axis):
        w = weight[unit]
        a, _, _, b, _, _ = spans(unit)
        half, plus, minus = (a, to_xp, to_xm) if axis == "x" else (b, to_zp, to_zm)
        send((unit, axis + "p1"), w.at[z, x, half], w.at[z, x, half], plus)
        send((unit, axis + "m1"), w.at[z, x, half], w.at[z, x, half], minus)

    def near_forward(unit, way):
        w = weight[unit]
        a, a0, a1, b, b0, b1 = spans(unit)
        at, half, part, device = {
            "xp": ((z, xm), a, a0, to_xp),
            "xm": ((z, xp), a, a1, to_xm),
            "zp": ((zm, x), b, b0, to_zp),
            "zm": ((zp, x), b, b1, to_zm),
        }[way]
        recv((unit, way + "1"), w.at[(*at, half)])
        send((unit, way + "f1"), w.at[(*at, part)], w.at[(*at, part)], device)

    places = {"z": (x, xm, xp, x2), "x": (z, zm, zp, z2)}

    def far_at(axis, row, i):
        return (row, places["z"][i]) if axis == "z" else (places["x"][i], row)

    def far_own(unit, axis, i):
        w = weight[unit]
        a, a0, a1, b, b0, b1 = spans(unit)
        if axis == "z":
            at, half, plus, minus = far_at("z", z, i), a, to_zp, to_zm
        else:
            at, half, plus, minus = far_at("x", x, i), b, to_xp, to_xm
        if i == 3:
            first, low, high = ("x", a0, a1) if axis == "z" else ("z", b0, b1)
            recv((unit, first + "pf1"), w.at[(*at, low)])
            recv((unit, first + "mf1"), w.at[(*at, high)])
        send((unit, axis + "p2", i), w.at[(*at, half)], w.at[(*at, half)], plus)
        send((unit, axis + "m2", i), w.at[(*at, half)], w.at[(*at, half)], minus)

    def far_forward(unit, way, i):
        w = weight[unit]
        a, a0, a1, b, b0, b1 = spans(unit)
        row, half, part, device = {
            "zp": (zm, a, a0, to_zp),
            "zm": (zp, a, a1, to_zm),
            "xp": (xm, b, b0, to_xp),
            "xm": (xp, b, b1, to_xm),
        }[way]
        at = far_at(way[0], row, i)
        recv((unit, way + "2", i), w.at[(*at, half)])
        send((unit, way + "f2", i), w.at[(*at, part)], w.at[(*at, part)], device)

    def weight_done(unit):
        w = weight[unit]
        a, a0, a1, b, b0, b1 = spans(unit)
        for i in range(4):
            recv((unit, "zpf2", i), w.at[(*far_at("z", z2, i), a0)])
            recv((unit, "zmf2", i), w.at[(*far_at("z", z2, i), a1)])
            recv((unit, "xpf2", i), w.at[(*far_at("x", x2, i), b0)])
            recv((unit, "xmf2", i), w.at[(*far_at("x", x2, i), b1)])

    mixer_bufs = (part1, pair1, sums1, fromp1, fromm1, relayp1, relaym1)
    ffn_bufs = (part2, pair2, sums2, fromp2, fromm2, relayp2, relaym2)

    def sum_pair(bufs, tag, ch):
        part, pair = bufs[:2]
        rows, _, _ = rows_of(ch)
        send((tag, "pair", ch), part.at[oc, :, rows], pair.at[:, rows], to_pt)

    def sum_start(bufs, tag, ch):
        part, pair, sums, fromp, fromm, relayp, relaym = bufs
        rows, low, high = rows_of(ch)
        half = pl.ds(128 * ch, 128)
        recv((tag, "pair", ch), pair.at[:, rows])
        for place in (y2, yp, ym):
            sums[place, rows] = (
                part[c, place, rows].astype(F32) + pair[place, rows].astype(F32)
            ).astype(BF16)
        send((tag, "rp", ch), sums.at[y2, low], relayp.at[half], to_yp)
        send((tag, "rm", ch), sums.at[y2, high], relaym.at[half], to_ym)
        send((tag, "op", ch), sums.at[yp, high], fromm.at[high], to_yp)
        send((tag, "om", ch), sums.at[ym, low], fromp.at[low], to_ym)

    def sum_relay(bufs, tag, ch, side):
        part, pair, sums, fromp, fromm, relayp, relaym = bufs
        rows, low, high = rows_of(ch)
        half = pl.ds(128 * ch, 128)
        if side == "a":
            recv((tag, "rp", ch), relayp.at[half])
            sums[yp, low] = (sums[yp, low].astype(F32) + relayp[half].astype(F32)).astype(BF16)
            send((tag, "sp", ch), sums.at[yp, low], fromm.at[low], to_yp)
        else:
            recv((tag, "rm", ch), relaym.at[half])
            sums[ym, high] = (sums[ym, high].astype(F32) + relaym[half].astype(F32)).astype(BF16)
            send((tag, "sm", ch), sums.at[ym, high], fromp.at[high], to_ym)

    def sum_end(bufs, tag, ch):
        part, pair, sums, fromp, fromm, relayp, relaym = bufs
        rows, low, high = rows_of(ch)
        recv((tag, "op", ch), fromm.at[high])
        recv((tag, "om", ch), fromp.at[low])
        recv((tag, "sp", ch), fromm.at[low])
        recv((tag, "sm", ch), fromp.at[high])
        return (part[c, y, rows].astype(F32) + pair[y, rows].astype(F32)) + (
            fromp[rows].astype(F32) + fromm[rows].astype(F32)
        )

    stores = []

    def mixer_end(ch):
        rows, _, _ = rows_of(ch)
        total = sum_end(mixer_bufs, "R", ch)
        resid[y, c, rows] = (tok[y, c, rows].astype(F32) + total).astype(BF16)

    def ffn_end(ch):
        rows, _, _ = rows_of(ch)
        total = sum_end(ffn_bufs, "V", ch)
        out_ref[rows, :] = (resid[y, c, rows].astype(F32) + total).astype(BF16)
        stores.append(local(out_ref.at[rows], out_hbm.at[rows]))

    def norm_rows(buf, gain, ch):
        def body(i, carry):
            rows = pl.ds(pl.multiple_of(SEQ * ch + 32 * i, 32), 32)
            blocks = [buf[p // 2, p % 2, rows].astype(F32) for p in range(8)]
            squares = blocks[0] * blocks[0]
            for block in blocks[1:]:
                squares = squares + block * block
            mean = jnp.sum(squares, axis=-1, keepdims=True) * (1.0 / 2048.0)
            factor = lax.rsqrt(mean + EPS)
            for p in range(8):
                lanes = slice(256 * p, 256 * p + 256)
                normed[rows, lanes] = (blocks[p] * factor * gain[:, lanes]).astype(BF16)
            return carry

        lax.fori_loop(0, 8, body, 0)

    def mixer(ch):
        rows, _, _ = rows_of(ch)
        qkv = dot(normed[rows, :], w_qo[:, :, :, 0:256].reshape(2048, 256))
        gate = dot(normed[rows, :], w_qo[:, :, :, 256:384].reshape(2048, 128))
        gate = gate.astype(BF16).astype(F32)
        qk = qkv[:, :128].astype(BF16).astype(F32)
        value = qkv[:, 128:].astype(BF16)
        lane = lax.broadcasted_iota(jnp.int32, (SEQ, 128), 1)
        turned = jnp.where(
            lax.rem(lane, 2) == 0, pltpu.roll(qk, 127, axis=1), pltpu.roll(qk, 1, axis=1)
        )
        rotated = qk * cos_ref[...] + turned * sin_ref[...]
        queries = jnp.where(lane < DK, rotated, 0.0).astype(BF16)
        keys = pltpu.roll(rotated, DK, axis=1).astype(BF16)
        scores = lax.dot_general(
            queries, keys, (((1,), (1,)), ((), ())), preferred_element_type=F32
        )
        retained = dot((scores * mask[...]).astype(BF16), value)
        center = jnp.mean(retained, axis=-1, keepdims=True)
        moved = retained - center
        spread = jnp.mean(moved * moved, axis=-1, keepdims=True)
        grouped = moved * lax.rsqrt(spread + EPS) * head_gain[...]
        mixed[rows] = (grouped * silu(gate)).astype(BF16)

    def mixer_out(ch):
        rows, _, _ = rows_of(ch)

        def body(p, carry):
            py, pc = lax.div(p, 2), lax.rem(p, 2)
            block = jnp.concatenate(
                [w_qo[py, 2 * pc, :, 384:512], w_qo[py, 2 * pc + 1, :, 384:512]], axis=1
            )
            part1[pc, py, rows] = dot(mixed[rows], block).astype(BF16)
            return carry

        lax.fori_loop(0, 8, body, 0)

    def gate_up(ch, first):
        rows, _, _ = rows_of(ch)

        def body(j, carry):
            columns = pl.ds(pl.multiple_of(256 * j, 256), 256)
            both = dot(normed[rows, :], w_gu[:, :, :, columns].reshape(2048, 256))
            hidden[rows, pl.ds(pl.multiple_of(128 * j, 128), 128)] = (
                silu(both[:, :128]) * both[:, 128:]
            ).astype(BF16)
            return carry

        if first:
            lax.fori_loop(0, 3, body, 0)
            return
        lax.fori_loop(3, 5, body, 0)
        both = dot(normed[rows, :], w_gu[:, :, :, 1280:1408].reshape(2048, 128))
        hidden[rows, 640:768] = (silu(both) * pltpu.roll(both, 64, axis=1)).astype(BF16)

    def down(ch, first):
        rows, _, _ = rows_of(ch)

        def body(p, carry):
            py, pc = lax.div(p, 2), lax.rem(p, 2)
            block = jnp.concatenate([w_d[py, 2 * pc], w_d[py, 2 * pc + 1]], axis=1)
            part2[pc, py, rows] = dot(hidden[rows, :704], block).astype(BF16)
            return carry

        lax.fori_loop(*((0, 4) if first else (4, 8)), body, 0)

    actions = {
        "ox": lambda u: near_own(u, "x"),
        "oz": lambda u: near_own(u, "z"),
        "e": weight_done,
        "stage_gu": stage_gate_up,
        "stage_d": stage_down,
        "stage_c": stage_rest,
        "Rc": mixer_end,
        "Vc": ffn_end,
        "norm1": lambda ch: norm_rows(tok, mix_gain, ch),
        "norm2": lambda ch: norm_rows(resid, ffn_gain, ch),
        "mixa": mixer,
        "mixb": mixer_out,
        "gua": functools.partial(gate_up, first=True),
        "gub": functools.partial(gate_up, first=False),
        "downa": functools.partial(down, first=True),
        "downb": functools.partial(down, first=False),
    }
    for way in ("xp", "xm", "zp", "zm"):
        actions["f" + way] = functools.partial(near_forward, way=way)
        for i in range(4):
            actions[f"h{i}" + way] = functools.partial(far_forward, way=way, i=i)
    for i in range(4):
        actions[f"g{i}z"] = functools.partial(far_own, axis="z", i=i)
        actions[f"g{i}x"] = functools.partial(far_own, axis="x", i=i)
    for tag, buf in (("T", tok), ("U", resid)):
        actions[tag + "p"] = functools.partial(gather_own, buf, tag)
        actions[tag + "fa"] = functools.partial(gather_forward, buf, tag, side="a")
        actions[tag + "fb"] = functools.partial(gather_forward, buf, tag, side="b")
        actions[tag + "g"] = functools.partial(gather_far, buf, tag)
        actions[tag + "d"] = functools.partial(gather_done, buf, tag)
    for tag, bufs in (("R", mixer_bufs), ("V", ffn_bufs)):
        actions[tag + "x"] = functools.partial(sum_pair, bufs, tag)
        actions[tag + "a"] = functools.partial(sum_start, bufs, tag)
        actions[tag + "ba"] = functools.partial(sum_relay, bufs, tag, side="a")
        actions[tag + "bb"] = functools.partial(sum_relay, bufs, tag, side="b")
    for entry in SCHEDULE:
        name, what = entry.split(".")
        actions[name](int(what) if what.isdigit() else what)

    for copy in sent:
        copy.wait_send()
    for copy in stores:
        copy.wait()
    assert len(ids) <= MAX_COPIES


def per_device(*args):
    (tokens, mix_gain, query_w, key_w, value_w, gate_w, out_w, head_gain, ffn_gain) = args[:9]
    ffn_gate, ffn_up, ffn_down = args[9:]
    cosine, sine = rope_tables()
    hbm = pl.BlockSpec(memory_space=pltpu.HBM)
    rows = tokens.shape[0]

    def sum_buffers():
        return [
            pltpu.VMEM((2, 4, rows, 256), BF16),
            pltpu.VMEM((4, rows, 256), BF16),
            pltpu.VMEM((4, rows, 256), BF16),
            pltpu.VMEM((rows, 256), BF16),
            pltpu.VMEM((rows, 256), BF16),
            pltpu.VMEM((rows // 2, 256), BF16),
            pltpu.VMEM((rows // 2, 256), BF16),
        ]

    call = pl.pallas_call(
        layer_kernel,
        out_shape=jax.ShapeDtypeStruct((rows, 256), BF16),
        in_specs=[hbm] * 15,
        out_specs=hbm,
        scratch_shapes=[
            pltpu.VMEM((4, 2, rows, 256), BF16),
            pltpu.VMEM((4, 2, rows, 256), BF16),
            pltpu.VMEM((rows, 2048), BF16),
            pltpu.VMEM((4, 4, 128, 512), BF16),
            pltpu.VMEM((4, 4, 128, 1408), BF16),
            pltpu.VMEM((4, 4, 704, 128), BF16),
            pltpu.VMEM((2 * DK, 128), BF16),
            pltpu.VMEM((1408, 128), BF16),
            pltpu.VMEM((1, 2048), F32),
            pltpu.VMEM((1, 2048), F32),
            pltpu.VMEM((1, DV), F32),
            pltpu.VMEM((SEQ, 128), F32),
            pltpu.VMEM((SEQ, 128), F32),
            pltpu.VMEM((HEADS, 8, 128), F32),
            pltpu.VMEM((rows, 256), BF16),
            pltpu.VMEM((SEQ, SEQ), F32),
            pltpu.VMEM((rows, DV), BF16),
            pltpu.VMEM((rows, 768), BF16),
            *sum_buffers(),
            *sum_buffers(),
            pltpu.SemaphoreType.DMA((32,)),
            pltpu.SemaphoreType.DMA((MAX_COPIES,)),
            pltpu.SemaphoreType.DMA((MAX_COPIES,)),
        ],
        compiler_params=pltpu.CompilerParams(
            collective_id=0, has_side_effects=True, vmem_limit_bytes=54 * 2**20
        ),
        cost_estimate=pl.CostEstimate(
            flops=11_000_000_000, bytes_accessed=4_000_000, transcendentals=1_000_000
        ),
        name="layer",
    )
    return call(
        tokens,
        mix_gain.reshape(1, -1),
        query_w.T,
        key_w.T,
        value_w,
        gate_w,
        out_w,
        head_gain,
        ffn_gain.reshape(1, -1),
        ffn_gate.T,
        ffn_up.T,
        ffn_down,
        jnp.asarray(cosine),
        jnp.asarray(sine),
        jnp.asarray(decay_table()),
    )


def solution(mesh):
    placed = (
        P(("rep", "fs"), "tp"),
        P(),
        P("fs", "tp"),
        P("fs", "tp"),
        P("fs", "tp"),
        P("fs", "tp"),
        P("tp", "fs"),
        P("tp", None),
        P(),
        P("fs", "tp"),
        P("fs", "tp"),
        P("tp", "fs"),
    )
    return jax.shard_map(
        per_device, mesh=mesh, in_specs=placed, out_specs=P(("rep", "fs"), "tp"), check_vma=False
    )
```

```python
import functools

import jax
import jax.numpy as jnp
import numpy as np
from jax import lax
from jax.experimental import pallas as pl
from jax.experimental.pallas import tpu as pltpu
from jax.sharding import PartitionSpec as P

HEADS = 8
DK = 64
DV = 128
SEQ = 256
EPS = 1e-06
ROPE_BASE = 10000.0
F32 = jnp.float32
BF16 = jnp.bfloat16
MESH = pl.DeviceIdType.MESH
RECEIVES = 179
SENDS = 14

UNITS = (
    (0, 64, 32, 64, 32),
    (0, 32, 16, 32, 16),
    (64, 32, 16, 32, 16),
    (0, 176, 96, 176, 96),
    (352, 176, 96, 176, 96),
)
WEIGHT_OF = (0, 1, 1, 2, 2)

SCHEDULE = (
    8, 0, 274, 48, 248, 275, 80, 10, 2, 272, 40, 32, 24, 16, 64, 96,
    282, 290, 144, 112, 176, 56, 208, 256, 88, 104, 72, 291, 9, 1, 283, 280,
    288, 273, 264, 192, 216, 120, 128, 184, 160, 224, 152, 298, 200, 232, 168, 136,
    82, 299, 4, 50, 26, 42, 34, 66, 306, 434, 18, 12, 33, 90, 307, 11,
    296, 435, 25, 41, 98, 58, 240, 443, 451, 355, 281, 304, 17, 289, 442, 106,
    450, 354, 363, 81, 74, 432, 210, 440, 297, 44, 362, 36, 448, 194, 130, 146,
    52, 352, 162, 305, 154, 114, 122, 3, 178, 35, 371, 379, 226, 218, 360, 43,
    202, 186, 433, 170, 138, 234, 378, 370, 20, 97, 57, 51, 441, 387, 65, 105,
    315, 449, 376, 19, 27, 353, 49, 28, 83, 242, 368, 89, 59, 386, 99, 68,
    314, 361, 108, 67, 323, 73, 107, 91, 75, 100, 384, 115, 153, 92, 217, 331,
    193, 76, 113, 60, 201, 233, 121, 225, 148, 322, 330, 377, 369, 84, 137, 161,
    169, 185, 312, 145, 177, 339, 236, 209, 228, 211, 171, 147, 187, 204, 129, 163,
    123, 227, 139, 219, 131, 155, 338, 195, 347, 179, 235, 220, 203, 164, 116, 132,
    385, 313, 346, 196, 124, 156, 172, 188, 180, 140, 459, 212, 458, 241, 320, 328,
    467, 466, 243, 475, 244, 483, 329, 321, 491, 395, 474, 336, 482, 490, 394, 403,
    344, 456, 464, 337, 402, 472, 480, 488, 392, 345, 457, 419, 411, 465, 400, 473,
    481, 489, 393, 418, 410, 427, 401, 408, 416, 426, 417, 409, 424, 425,
)


def rope_tables():
    half = DK // 2
    frequency = ROPE_BASE ** (-np.linspace(0.0, 1.0, half))
    angles = np.arange(SEQ)[:, None] * frequency[None, :]
    cosine = np.repeat(np.cos(angles), 2, axis=1)
    sine = np.repeat(np.sin(angles), 2, axis=1) * np.tile([-1.0, 1.0], half)
    scale = DK**-0.5
    return (
        np.concatenate([cosine, cosine * scale], axis=1).astype(np.float32),
        np.concatenate([sine, sine * scale], axis=1).astype(np.float32),
    )


def decay_table():
    rates = np.log1p(-np.exp2(-5.0 - 4.0 * np.arange(HEADS) / (HEADS - 1)))
    return np.broadcast_to(rates[:, None, None], (HEADS, 8, 128)).astype(np.float32)


def silu(values):
    return values / (1.0 + jnp.exp(-values))


def dot(left, right):
    return jnp.dot(left, right, preferred_element_type=F32)


def layer_kernel(
    tok_hbm,
    mix_gain_hbm,
    query_hbm,
    key_hbm,
    value_hbm,
    gate_hbm,
    out_w_hbm,
    head_gain_hbm,
    ffn_gain_hbm,
    ffn_gate_hbm,
    ffn_up_hbm,
    down_hbm,
    cos_hbm,
    sin_hbm,
    rate_hbm,
    out_hbm,
    tok,
    resid,
    normed,
    w_qo,
    w_gu,
    w_d,
    turn_qk,
    turn_gu,
    mix_gain,
    ffn_gain,
    head_gain,
    cos_ref,
    sin_ref,
    rate_ref,
    out_ref,
    mask,
    mixed,
    hidden,
    part1,
    pair1,
    sums1,
    ends1,
    relay1,
    part2,
    pair2,
    sums2,
    ends2,
    relay2,
    local_sem,
    send_sem,
    recv_sem,
):
    rep, fs, tp = lax.axis_index("rep"), lax.axis_index("fs"), lax.axis_index("tp")
    y, c = lax.div(tp, 2), lax.rem(tp, 2)
    z, x = lax.div(fs, 4), lax.rem(fs, 4)
    oc = 1 - c

    def step(value, by, size):
        return lax.rem(value + by, size)

    yp, y2, ym = step(y, 1, 4), step(y, 2, 4), step(y, 3, 4)
    xp, x2, xm = step(x, 1, 4), step(x, 2, 4), step(x, 3, 4)
    zp, z2, zm = step(z, 1, 4), step(z, 2, 4), step(z, 3, 4)
    zall = rep * 4 + z

    def z_device(place):
        return (lax.div(place, 4), lax.rem(place, 4) * 4 + x, tp)

    to_yp, to_ym = (rep, fs, yp * 2 + c), (rep, fs, ym * 2 + c)
    to_pt = (rep, fs, y * 2 + oc)
    to_xp, to_xm = (rep, z * 4 + xp, tp), (rep, z * 4 + xm, tp)
    to_zp, to_zm = z_device(step(zall, 1, 8)), z_device(step(zall, 7, 8))

    barrier = pltpu.get_barrier_semaphore()
    peers = (to_yp, to_ym, to_pt, to_xp, to_xm, to_zp, to_zm)
    for peer in peers:
        pl.semaphore_signal(barrier, inc=1, device_id=peer, device_id_type=MESH)

    ids = {}
    groups = {}

    def send(group, key, src, dst, device):
        k = ids.setdefault(key, len(ids))
        g = groups.setdefault(group, len(groups))
        pltpu.make_async_remote_copy(
            src_ref=src,
            dst_ref=dst,
            send_sem=send_sem.at[g],
            recv_sem=recv_sem.at[k],
            device_id=device,
            device_id_type=MESH,
        ).start()

    def recv(key, dst):
        pltpu.make_async_remote_copy(
            src_ref=dst,
            dst_ref=dst,
            send_sem=send_sem.at[0],
            recv_sem=recv_sem.at[ids[key]],
            device_id=to_pt,
            device_id_type=MESH,
        ).wait_recv()

    def all_sent(group, src):
        pltpu.make_async_remote_copy(
            src_ref=src,
            dst_ref=src,
            send_sem=send_sem.at[groups[group]],
            recv_sem=recv_sem.at[0],
            device_id=to_pt,
            device_id_type=MESH,
        ).wait_send()

    count = [0]

    def local(src, dst):
        copy = pltpu.make_async_copy(src, dst, local_sem.at[count[0]])
        count[0] += 1
        copy.start()
        return copy

    load_qk = [
        local(query_hbm, turn_qk.at[pl.ds(0, DK)]),
        local(key_hbm, turn_qk.at[pl.ds(DK, DK)]),
    ]
    load_vgo = [
        local(value_hbm, w_qo.at[z, x, :, pl.ds(128, 128)]),
        local(gate_hbm, w_qo.at[z, x, :, pl.ds(256, 128)]),
        local(out_w_hbm, w_qo.at[z, x, :, pl.ds(384, 128)]),
    ]
    load_tok = [local(tok_hbm, tok.at[y, c])]
    load_gu = []
    for j in range(6):
        width = 128 if j < 5 else 64
        for k, source in enumerate((ffn_gate_hbm, ffn_up_hbm)):
            place = pl.ds(256 * j + width * k, width)
            load_gu.append(local(source.at[pl.ds(128 * j, width)], turn_gu.at[place]))
    load_down = [local(down_hbm, w_d.at[z, x])]
    load_rest = [
        local(mix_gain_hbm, mix_gain),
        local(ffn_gain_hbm, ffn_gain),
        local(head_gain_hbm, head_gain),
        local(cos_hbm, cos_ref),
        local(sin_hbm, sin_ref),
        local(rate_hbm, rate_ref),
    ]

    def loaded(copies):
        for copy in copies:
            copy.wait()

    loaded(load_qk)
    w_qo[z, x, :, 0:128] = turn_qk[...].T
    loaded(load_vgo)
    loaded(load_tok)
    pl.semaphore_wait(barrier, len(peers))

    def stage_gate_up(_):
        loaded(load_gu)
        for j in range(11):
            lanes = slice(128 * j, 128 * j + 128)
            w_gu[z, x, :, lanes] = turn_gu[lanes, :].T

    def stage_down(_):
        loaded(load_down)

    def stage_rest(_):
        loaded(load_rest)
        gap = lax.broadcasted_iota(jnp.int32, (SEQ, 128), 0) - lax.broadcasted_iota(
            jnp.int32, (SEQ, 128), 1
        )
        rate = rate_ref[tp][:1, :]
        for half in range(2):
            distance = (gap - 128 * half).astype(F32)
            mask[:, 128 * half : 128 * half + 128] = jnp.where(
                distance >= 0.0, jnp.exp(jnp.maximum(distance, 0.0) * rate), 0.0
            )

    def rows_of(ch):
        return pl.ds(SEQ * ch, SEQ), pl.ds(SEQ * ch, 128), pl.ds(SEQ * ch + 128, 128)

    def gather_own(buf, tag, ch):
        rows, _, _ = rows_of(ch)
        own = buf.at[y, c, rows]
        send((tag, 0), (tag, 0, ch), own, own, to_yp)
        send((tag, 0), (tag, 1, ch), own, own, to_ym)
        send((tag, 1), (tag, 3, ch), own, own, to_pt)

    def gather_forward(buf, tag, ch, side):
        rows, low, high = rows_of(ch)
        row, part, device = ((ym, low, to_yp), (yp, high, to_ym))[side]
        recv((tag, side, ch), buf.at[row, c, rows])
        send((tag, 0), (tag, 2, ch), buf.at[row, c, part], buf.at[row, c, part], device)
        send((tag, 1), (tag, 3, ch), buf.at[row, c, rows], buf.at[row, c, rows], to_pt)

    def gather_far(buf, tag, ch):
        rows, _, _ = rows_of(ch)
        recv((tag, 2, ch), buf.at[y2, c, rows])
        send((tag, 1), (tag, 3, ch), buf.at[y2, c, rows], buf.at[y2, c, rows], to_pt)

    def gather_done(buf, tag, ch):
        rows, _, _ = rows_of(ch)
        recv((tag, 3, ch), buf.at[:, oc, rows])

    buffers = (w_qo, w_gu, w_gu, w_d, w_d)

    def spans(unit):
        first, a, a0, b, b0 = UNITS[unit]
        half_a = (pl.ds(first, a), pl.ds(first, a0), pl.ds(first + a0, a - a0))
        first = first + a
        return half_a, (pl.ds(first, b), pl.ds(first, b0), pl.ds(first + b0, b - b0))

    near = ((xm, xp), (zm, zp))
    far = (x2, z2)
    devices = ((to_xp, to_xm), (to_zp, to_zm))

    def near_at(axis, place):
        return (z, place) if axis == 0 else (place, x)

    def near_own(unit, axis):
        w, name = buffers[unit], WEIGHT_OF[unit]
        half = spans(unit)[axis][0]
        own = w.at[z, x, half]
        for way in range(2):
            send((name, 0), (unit, 0, axis, way), own, own, devices[axis][way])

    def near_forward(unit, axis, way):
        w, name = buffers[unit], WEIGHT_OF[unit]
        at = near_at(axis, near[axis][way])
        half = spans(unit)[axis]
        recv((unit, 0, axis, way), w.at[(*at, half[0])])
        part = w.at[(*at, half[1 + way])]
        send((name, 0), (unit, 1, axis), part, part, devices[axis][way])

    crossed = ((x, xm, xp, x2), (z, zm, zp, z2))

    def far_at(axis, place, i):
        return (place, crossed[0][i]) if axis == 0 else (crossed[1][i], place)

    def far_own(unit, axis, i):
        w, name = buffers[unit], WEIGHT_OF[unit]
        half = spans(unit)[axis][0]
        block = w.at[(*far_at(axis, (z, x)[axis], i), half)]
        if i == 3:
            recv((unit, 1, axis), block)
        for way in range(2):
            send((name, 1), (unit, 2, axis, way, i), block, block, devices[1 - axis][way])

    def far_forward(unit, axis, way, i):
        w, name = buffers[unit], WEIGHT_OF[unit]
        at = far_at(axis, near[1 - axis][way], i)
        half = spans(unit)[axis]
        recv((unit, 2, axis, way, i), w.at[(*at, half[0])])
        part = w.at[(*at, half[1 + way])]
        send((name, 1), (unit, 3), part, part, devices[1 - axis][way])

    def weight_done(unit):
        first, a, _, b, _ = UNITS[unit]
        recv((unit, 3), buffers[unit].at[0, :, pl.ds(first, a + b)])

    mixer_bufs = (part1, pair1, sums1, ends1, relay1)
    ffn_bufs = (part2, pair2, sums2, ends2, relay2)

    def sum_pair(bufs, tag, ch):
        part, pair = bufs[:2]
        rows, _, _ = rows_of(ch)
        send((tag, 1), (tag, 0, ch), part.at[oc, :, rows], pair.at[:, rows], to_pt)

    def sum_start(bufs, tag, ch):
        part, pair, sums, ends, relay = bufs
        rows, low, high = rows_of(ch)
        half = pl.ds(128 * ch, 128)
        recv((tag, 0, ch), pair.at[:, rows])
        for place in (y2, yp, ym):
            sums[place, rows] = (
                part[c, place, rows].astype(F32) + pair[place, rows].astype(F32)
            ).astype(BF16)
        send((tag, 0), (tag, 1, ch), sums.at[y2, low], relay.at[0, half], to_yp)
        send((tag, 0), (tag, 2, ch), sums.at[y2, high], relay.at[1, half], to_ym)
        send((tag, 0), (tag, 3, ch), sums.at[yp, high], ends.at[1, high], to_yp)
        send((tag, 0), (tag, 3, ch), sums.at[ym, low], ends.at[0, low], to_ym)

    def sum_relay(bufs, tag, ch, side):
        _, _, sums, ends, relay = bufs
        _, low, high = rows_of(ch)
        half = pl.ds(128 * ch, 128)
        place, part, device = ((yp, low, to_yp), (ym, high, to_ym))[side]
        recv((tag, 1 + side, ch), relay.at[side, half])
        sums[place, part] = (
            sums[place, part].astype(F32) + relay[side, half].astype(F32)
        ).astype(BF16)
        send((tag, 0), (tag, 3, ch), sums.at[place, part], ends.at[1 - side, part], device)

    def sum_end(bufs, tag, ch):
        part, pair, _, ends, _ = bufs
        rows, _, _ = rows_of(ch)
        recv((tag, 3, ch), ends.at[:, rows])
        return (part[c, y, rows].astype(F32) + pair[y, rows].astype(F32)) + (
            ends[0, rows].astype(F32) + ends[1, rows].astype(F32)
        )

    stores = []

    def mixer_end(ch):
        rows, _, _ = rows_of(ch)
        total = sum_end(mixer_bufs, 12, ch)
        resid[y, c, rows] = (tok[y, c, rows].astype(F32) + total).astype(BF16)

    def ffn_end(ch):
        rows, _, _ = rows_of(ch)
        total = sum_end(ffn_bufs, 13, ch)
        out_ref[rows, :] = (resid[y, c, rows].astype(F32) + total).astype(BF16)
        stores.append(local(out_ref.at[rows], out_hbm.at[rows]))

    def norm_rows(buf, gain, ch):
        def body(i, carry):
            rows = pl.ds(pl.multiple_of(SEQ * ch + 32 * i, 32), 32)
            blocks = [buf[p // 2, p % 2, rows].astype(F32) for p in range(8)]
            squares = blocks[0] * blocks[0]
            for block in blocks[1:]:
                squares = squares + block * block
            mean = jnp.sum(squares, axis=-1, keepdims=True) * (1.0 / 2048.0)
            factor = lax.rsqrt(mean + EPS)
            for p in range(8):
                lanes = slice(256 * p, 256 * p + 256)
                normed[rows, lanes] = (blocks[p] * factor * gain[:, lanes]).astype(BF16)
            return carry

        lax.fori_loop(0, 8, body, 0)

    def mixer(ch):
        rows, _, _ = rows_of(ch)
        qkv = dot(normed[rows, :], w_qo[:, :, :, 0:256].reshape(2048, 256))
        gate = dot(normed[rows, :], w_qo[:, :, :, 256:384].reshape(2048, 128))
        gate = gate.astype(BF16).astype(F32)
        qk = qkv[:, :128].astype(BF16).astype(F32)
        value = qkv[:, 128:].astype(BF16)
        lane = lax.broadcasted_iota(jnp.int32, (SEQ, 128), 1)
        turned = jnp.where(
            lax.rem(lane, 2) == 0, pltpu.roll(qk, 127, axis=1), pltpu.roll(qk, 1, axis=1)
        )
        rotated = qk * cos_ref[...] + turned * sin_ref[...]
        queries = jnp.where(lane < DK, rotated, 0.0).astype(BF16)
        keys = pltpu.roll(rotated, DK, axis=1).astype(BF16)
        scores = lax.dot_general(
            queries, keys, (((1,), (1,)), ((), ())), preferred_element_type=F32
        )
        retained = dot((scores * mask[...]).astype(BF16), value)
        center = jnp.mean(retained, axis=-1, keepdims=True)
        moved = retained - center
        spread = jnp.mean(moved * moved, axis=-1, keepdims=True)
        grouped = moved * lax.rsqrt(spread + EPS) * head_gain[...]
        mixed[rows] = (grouped * silu(gate)).astype(BF16)

    def mixer_out(ch):
        rows, _, _ = rows_of(ch)

        def body(p, carry):
            py, pc = lax.div(p, 2), lax.rem(p, 2)
            block = jnp.concatenate(
                [w_qo[py, 2 * pc, :, 384:512], w_qo[py, 2 * pc + 1, :, 384:512]], axis=1
            )
            part1[pc, py, rows] = dot(mixed[rows], block).astype(BF16)
            return carry

        lax.fori_loop(0, 8, body, 0, unroll=True)

    def gate_up(ch, first):
        rows, _, _ = rows_of(ch)

        def body(j, carry):
            columns = pl.ds(pl.multiple_of(256 * j, 256), 256)
            both = dot(normed[rows, :], w_gu[:, :, :, columns].reshape(2048, 256))
            hidden[rows, pl.ds(pl.multiple_of(128 * j, 128), 128)] = (
                silu(both[:, :128]) * both[:, 128:]
            ).astype(BF16)
            return carry

        if first:
            lax.fori_loop(0, 3, body, 0, unroll=True)
            return
        lax.fori_loop(3, 5, body, 0, unroll=True)
        both = dot(normed[rows, :], w_gu[:, :, :, 1280:1408].reshape(2048, 128))
        hidden[rows, 640:768] = (silu(both) * pltpu.roll(both, 64, axis=1)).astype(BF16)

    def down(ch, first):
        rows, _, _ = rows_of(ch)

        def body(p, carry):
            py, pc = lax.div(p, 2), lax.rem(p, 2)
            block = jnp.concatenate([w_d[py, 2 * pc], w_d[py, 2 * pc + 1]], axis=1)
            part2[pc, py, rows] = dot(hidden[rows, :704], block).astype(BF16)
            return carry

        lax.fori_loop(*((0, 4) if first else (4, 8)), body, 0, unroll=True)

    part = functools.partial
    actions = [part(near_own, axis=axis) for axis in range(2)]
    actions += [part(near_forward, axis=k // 2, way=k % 2) for k in range(4)]
    actions += [part(far_own, axis=k // 4, i=k % 4) for k in range(8)]
    actions += [part(far_forward, axis=k // 8, way=k // 4 % 2, i=k % 4) for k in range(16)]
    actions += [weight_done, stage_gate_up, stage_down, stage_rest]
    for tag, buf in ((10, tok), (11, resid)):
        actions.append(part(gather_own, buf, tag))
        actions += [part(gather_forward, buf, tag, side=side) for side in range(2)]
        actions += [part(gather_far, buf, tag), part(gather_done, buf, tag)]
    for tag, bufs, end in ((12, mixer_bufs, mixer_end), (13, ffn_bufs, ffn_end)):
        actions += [part(sum_pair, bufs, tag), part(sum_start, bufs, tag)]
        actions += [part(sum_relay, bufs, tag, side=side) for side in range(2)]
        actions.append(end)
    actions += [part(norm_rows, tok, mix_gain), mixer, mixer_out]
    actions += [part(norm_rows, resid, ffn_gain)]
    actions += [part(gate_up, first=True), part(gate_up, first=False)]
    actions += [part(down, first=True), part(down, first=False)]
    for code in SCHEDULE:
        actions[code // 8](code % 8)

    for name, w in enumerate((w_qo, w_gu, w_d)):
        all_sent((name, 0), w.at[0, pl.ds(0, 3)])
        all_sent((name, 1), w.at[pl.ds(0, 3)])
    for tag, buf in ((10, tok), (11, resid)):
        all_sent((tag, 0), buf.at[pl.ds(0, 3), 0])
        all_sent((tag, 1), buf.at[:, 0])
    for tag, bufs in ((12, mixer_bufs), (13, ffn_bufs)):
        all_sent((tag, 0), bufs[2].at[pl.ds(0, 3)])
        all_sent((tag, 1), bufs[0].at[0])
    for copy in stores:
        copy.wait()
    assert len(ids) == RECEIVES and len(groups) == SENDS


def per_device(*args):
    (tokens, mix_gain, query_w, key_w, value_w, gate_w, out_w, head_gain, ffn_gain) = args[:9]
    ffn_gate, ffn_up, ffn_down = args[9:]
    cosine, sine = rope_tables()
    hbm = pl.BlockSpec(memory_space=pltpu.HBM)
    rows = tokens.shape[0]

    def sum_buffers():
        return [
            pltpu.VMEM((2, 4, rows, 256), BF16),
            pltpu.VMEM((4, rows, 256), BF16),
            pltpu.VMEM((4, rows, 256), BF16),
            pltpu.VMEM((2, rows, 256), BF16),
            pltpu.VMEM((2, rows // 2, 256), BF16),
        ]

    call = pl.pallas_call(
        layer_kernel,
        out_shape=jax.ShapeDtypeStruct((rows, 256), BF16),
        in_specs=[hbm] * 15,
        out_specs=hbm,
        scratch_shapes=[
            pltpu.VMEM((4, 2, rows, 256), BF16),
            pltpu.VMEM((4, 2, rows, 256), BF16),
            pltpu.VMEM((rows, 2048), BF16),
            pltpu.VMEM((4, 4, 128, 512), BF16),
            pltpu.VMEM((4, 4, 128, 1408), BF16),
            pltpu.VMEM((4, 4, 704, 128), BF16),
            pltpu.VMEM((2 * DK, 128), BF16),
            pltpu.VMEM((1408, 128), BF16),
            pltpu.VMEM((1, 2048), F32),
            pltpu.VMEM((1, 2048), F32),
            pltpu.VMEM((1, DV), F32),
            pltpu.VMEM((SEQ, 128), F32),
            pltpu.VMEM((SEQ, 128), F32),
            pltpu.VMEM((HEADS, 8, 128), F32),
            pltpu.VMEM((rows, 256), BF16),
            pltpu.VMEM((SEQ, SEQ), F32),
            pltpu.VMEM((rows, DV), BF16),
            pltpu.VMEM((rows, 768), BF16),
            *sum_buffers(),
            *sum_buffers(),
            pltpu.SemaphoreType.DMA((32,)),
            pltpu.SemaphoreType.DMA((SENDS,)),
            pltpu.SemaphoreType.DMA((RECEIVES,)),
        ],
        compiler_params=pltpu.CompilerParams(
            collective_id=0, has_side_effects=True, vmem_limit_bytes=54 * 2**20
        ),
        cost_estimate=pl.CostEstimate(
            flops=11_000_000_000, bytes_accessed=4_000_000, transcendentals=1_000_000
        ),
        name="layer",
    )
    return call(
        tokens,
        mix_gain.reshape(1, -1),
        query_w.T,
        key_w.T,
        value_w,
        gate_w,
        out_w,
        head_gain,
        ffn_gain.reshape(1, -1),
        ffn_gate.T,
        ffn_up.T,
        ffn_down,
        jnp.asarray(cosine),
        jnp.asarray(sine),
        jnp.asarray(decay_table()),
    )


def solution(mesh):
    placed = (
        P(("rep", "fs"), "tp"),
        P(),
        P("fs", "tp"),
        P("fs", "tp"),
        P("fs", "tp"),
        P("fs", "tp"),
        P("tp", "fs"),
        P("tp", None),
        P(),
        P("fs", "tp"),
        P("fs", "tp"),
        P("tp", "fs"),
    )
    return jax.shard_map(
        per_device, mesh=mesh, in_specs=placed, out_specs=P(("rep", "fs"), "tp"), check_vma=False
    )
```

```python
import functools

import jax
import jax.numpy as jnp
import numpy as np
from jax import lax
from jax.experimental import pallas as pl
from jax.experimental.pallas import tpu as pltpu
from jax.sharding import PartitionSpec as P

HEADS = 8
DK = 64
DV = 128
SEQ = 256
EPS = 1e-06
ROPE_BASE = 10000.0
F32 = jnp.float32
BF16 = jnp.bfloat16
MESH = pl.DeviceIdType.MESH
RECEIVES = 195
SENDS = 18

UNITS = (
    (0, 64, 32, 64, 32),
    (0, 32, 16, 32, 16),
    (64, 32, 16, 32, 16),
    (0, 176, 96, 176, 96),
    (0, 176, 96, 176, 96),
)
WEIGHT_OF = (0, 1, 1, 2, 3)

SCHEDULE = (
    0, 8, 273, 80, 48, 248, 272, 256, 274, 1, 9, 24, 16, 40, 32, 96,
    56, 88, 289, 281, 264, 64, 11, 3, 288, 280, 72, 104, 275, 2, 10, 160,
    290, 208, 192, 112, 176, 144, 184, 216, 224, 152, 297, 120, 282, 128, 296, 168,
    136, 200, 232, 305, 12, 27, 35, 67, 19, 33, 4, 43, 51, 91, 473, 59,
    304, 49, 18, 41, 25, 472, 99, 283, 17, 83, 291, 65, 97, 26, 50, 89,
    240, 480, 488, 352, 298, 481, 489, 299, 353, 360, 306, 107, 474, 482, 307, 81,
    75, 361, 490, 147, 42, 57, 82, 195, 354, 115, 34, 475, 483, 376, 368, 491,
    179, 235, 155, 123, 211, 203, 362, 163, 139, 355, 171, 227, 131, 187, 219, 66,
    105, 44, 377, 73, 58, 369, 98, 90, 113, 129, 384, 312, 106, 243, 74, 209,
    378, 177, 217, 185, 161, 121, 370, 363, 385, 145, 201, 153, 137, 225, 193, 36,
    169, 178, 536, 328, 320, 130, 114, 20, 146, 313, 233, 386, 154, 186, 28, 210,
    202, 379, 194, 234, 371, 218, 122, 226, 138, 170, 162, 84, 314, 60, 336, 241,
    344, 76, 92, 68, 496, 52, 100, 321, 108, 329, 387, 315, 242, 504, 512, 322,
    212, 188, 180, 330, 140, 164, 124, 337, 228, 220, 172, 156, 196, 132, 520, 116,
    204, 236, 148, 392, 345, 497, 505, 323, 331, 400, 513, 338, 521, 393, 244, 537,
    528, 346, 432, 529, 433, 401, 498, 506, 339, 440, 514, 522, 394, 416, 408, 347,
    441, 530, 434, 499, 409, 417, 402, 507, 442, 515, 523, 395, 424, 448, 456, 531,
    435, 457, 449, 425, 403, 443, 418, 410, 450, 458, 464, 465, 411, 419, 459, 451,
    426, 466, 427, 467,
)


def rope_tables():
    half = DK // 2
    frequency = ROPE_BASE ** (-np.linspace(0.0, 1.0, half))
    angles = np.arange(SEQ)[:, None] * frequency[None, :]
    cosine = np.repeat(np.cos(angles), 2, axis=1)
    sine = np.repeat(np.sin(angles), 2, axis=1) * np.tile([-1.0, 1.0], half)
    scale = DK**-0.5
    return (
        np.concatenate([cosine, cosine * scale], axis=1).astype(np.float32),
        np.concatenate([sine, sine * scale], axis=1).astype(np.float32),
    )


def decay_table():
    rates = np.log1p(-np.exp2(-5.0 - 4.0 * np.arange(HEADS) / (HEADS - 1)))
    return np.broadcast_to(rates[:, None, None], (HEADS, 8, 128)).astype(np.float32)


def silu(values):
    return values / (1.0 + jnp.exp(-values))


def dot(left, right):
    return jnp.dot(left, right, preferred_element_type=F32)


def layer_kernel(
    tok_hbm,
    mix_gain_hbm,
    query_hbm,
    key_hbm,
    value_hbm,
    gate_hbm,
    out_w_hbm,
    head_gain_hbm,
    ffn_gain_hbm,
    ffn_gate_hbm,
    ffn_up_hbm,
    down_hbm,
    cos_hbm,
    sin_hbm,
    rate_hbm,
    out_ref,
    tok,
    resid,
    normed,
    w_qo,
    w_gu,
    w_d0,
    w_d1,
    joined,
    down_in,
    turn_qk,
    turn_gu,
    mix_gain,
    ffn_gain,
    head_gain,
    cos_ref,
    sin_ref,
    rate_ref,
    mask,
    mixed,
    hidden,
    part1,
    pair1,
    sums1,
    ends1,
    relay1,
    part2,
    pair2,
    sums2,
    ends2,
    relay2,
    part3,
    pair3,
    sums3,
    ends3,
    relay3,
    first,
    local_sem,
    send_sem,
    recv_sem,
):
    rep, fs, tp = lax.axis_index("rep"), lax.axis_index("fs"), lax.axis_index("tp")
    y, c = lax.div(tp, 2), lax.rem(tp, 2)
    z, x = lax.div(fs, 4), lax.rem(fs, 4)
    oc = 1 - c

    def step(value, by, size):
        return lax.rem(value + by, size)

    yp, y2, ym = step(y, 1, 4), step(y, 2, 4), step(y, 3, 4)
    xp, x2, xm = step(x, 1, 4), step(x, 2, 4), step(x, 3, 4)
    zp, z2, zm = step(z, 1, 4), step(z, 2, 4), step(z, 3, 4)
    zall = rep * 4 + z

    def z_device(place):
        return (lax.div(place, 4), lax.rem(place, 4) * 4 + x, tp)

    to_yp, to_ym = (rep, fs, yp * 2 + c), (rep, fs, ym * 2 + c)
    to_pt = (rep, fs, y * 2 + oc)
    to_xp, to_xm = (rep, z * 4 + xp, tp), (rep, z * 4 + xm, tp)
    to_zp, to_zm = z_device(step(zall, 1, 8)), z_device(step(zall, 7, 8))

    barrier = pltpu.get_barrier_semaphore()
    peers = (to_yp, to_ym, to_pt, to_xp, to_xm, to_zp, to_zm)
    for peer in peers:
        pl.semaphore_signal(barrier, inc=1, device_id=peer, device_id_type=MESH)

    ids = {}
    groups = {}

    def send(group, key, src, dst, device):
        k = ids.setdefault(key, len(ids))
        g = groups.setdefault(group, len(groups))
        pltpu.make_async_remote_copy(
            src_ref=src,
            dst_ref=dst,
            send_sem=send_sem.at[g],
            recv_sem=recv_sem.at[k],
            device_id=device,
            device_id_type=MESH,
        ).start()

    def recv(key, dst):
        pltpu.make_async_remote_copy(
            src_ref=dst,
            dst_ref=dst,
            send_sem=send_sem.at[0],
            recv_sem=recv_sem.at[ids[key]],
            device_id=to_pt,
            device_id_type=MESH,
        ).wait_recv()

    def all_sent(group, src):
        pltpu.make_async_remote_copy(
            src_ref=src,
            dst_ref=src,
            send_sem=send_sem.at[groups[group]],
            recv_sem=recv_sem.at[0],
            device_id=to_pt,
            device_id_type=MESH,
        ).wait_send()

    count = [0]

    def local(src, dst):
        copy = pltpu.make_async_copy(src, dst, local_sem.at[count[0]])
        count[0] += 1
        copy.start()
        return copy

    load_qk = [
        local(query_hbm, turn_qk.at[pl.ds(0, DK)]),
        local(key_hbm, turn_qk.at[pl.ds(DK, DK)]),
    ]
    load_vgo = [
        local(value_hbm, w_qo.at[z, x, :, pl.ds(128, 128)]),
        local(gate_hbm, w_qo.at[z, x, :, pl.ds(256, 128)]),
        local(out_w_hbm, w_qo.at[z, x, :, pl.ds(384, 128)]),
    ]
    load_tok = [local(tok_hbm, tok.at[y, c])]
    load_gu = []
    for j in range(6):
        width = 128 if j < 5 else 64
        for k, source in enumerate((ffn_gate_hbm, ffn_up_hbm)):
            place = pl.ds(256 * j + width * k, width)
            load_gu.append(local(source.at[pl.ds(128 * j, width)], turn_gu.at[place]))
    load_down = [local(down_hbm, down_in)]
    load_rest = [
        local(mix_gain_hbm, mix_gain),
        local(ffn_gain_hbm, ffn_gain),
        local(head_gain_hbm, head_gain),
        local(cos_hbm, cos_ref),
        local(sin_hbm, sin_ref),
        local(rate_hbm, rate_ref),
    ]

    def loaded(copies):
        for copy in copies:
            copy.wait()

    loaded(load_qk)
    w_qo[z, x, :, 0:128] = turn_qk[...].T
    loaded(load_vgo)
    loaded(load_tok)
    pl.semaphore_wait(barrier, len(peers))

    def stage_gate_up(_):
        loaded(load_gu)
        for j in range(11):
            lanes = slice(128 * j, 128 * j + 128)
            w_gu[z, x, :, lanes] = turn_gu[lanes, :].T

    def stage_down(_):
        loaded(load_down)
        top, low = down_in[0:352, :], down_in[352:704, :]
        w_d0[z, x] = jnp.concatenate([top[:, :64], low[:, :64]], axis=1)
        w_d1[z, x] = jnp.concatenate([top[:, 64:], low[:, 64:]], axis=1)

    def stage_rest(_):
        loaded(load_rest)
        gap = lax.broadcasted_iota(jnp.int32, (SEQ, 128), 0) - lax.broadcasted_iota(
            jnp.int32, (SEQ, 128), 1
        )
        rate = rate_ref[tp][:1, :]
        for half in range(2):
            distance = (gap - 128 * half).astype(F32)
            mask[:, 128 * half : 128 * half + 128] = jnp.where(
                distance >= 0.0, jnp.exp(jnp.maximum(distance, 0.0) * rate), 0.0
            )

    def rows_of(ch):
        return pl.ds(SEQ * ch, SEQ), pl.ds(SEQ * ch, 128), pl.ds(SEQ * ch + 128, 128)

    def gather_own(buf, tag, ch):
        rows, _, _ = rows_of(ch)
        own = buf.at[y, c, rows]
        send((tag, 0), (tag, 0, ch), own, own, to_yp)
        send((tag, 0), (tag, 1, ch), own, own, to_ym)
        send((tag, 1), (tag, 3, ch), own, own, to_pt)

    def gather_forward(buf, tag, ch, side):
        rows, low, high = rows_of(ch)
        row, part, device = ((ym, low, to_yp), (yp, high, to_ym))[side]
        recv((tag, side, ch), buf.at[row, c, rows])
        send((tag, 0), (tag, 2, ch), buf.at[row, c, part], buf.at[row, c, part], device)
        send((tag, 1), (tag, 3, ch), buf.at[row, c, rows], buf.at[row, c, rows], to_pt)

    def gather_far(buf, tag, ch):
        rows, _, _ = rows_of(ch)
        recv((tag, 2, ch), buf.at[y2, c, rows])
        send((tag, 1), (tag, 3, ch), buf.at[y2, c, rows], buf.at[y2, c, rows], to_pt)

    def gather_done(buf, tag, ch):
        rows, _, _ = rows_of(ch)
        recv((tag, 3, ch), buf.at[:, oc, rows])

    buffers = (w_qo, w_gu, w_gu, w_d0, w_d1)

    def spans(unit):
        first, a, a0, b, b0 = UNITS[unit]
        half_a = (pl.ds(first, a), pl.ds(first, a0), pl.ds(first + a0, a - a0))
        first = first + a
        return half_a, (pl.ds(first, b), pl.ds(first, b0), pl.ds(first + b0, b - b0))

    near = ((xm, xp), (zm, zp))
    far = (x2, z2)
    devices = ((to_xp, to_xm), (to_zp, to_zm))

    def near_at(axis, place):
        return (z, place) if axis == 0 else (place, x)

    def near_own(unit, axis):
        w, name = buffers[unit], WEIGHT_OF[unit]
        half = spans(unit)[axis][0]
        own = w.at[z, x, half]
        for way in range(2):
            send((name, 0), (unit, 0, axis, way), own, own, devices[axis][way])

    def near_forward(unit, axis, way):
        w, name = buffers[unit], WEIGHT_OF[unit]
        at = near_at(axis, near[axis][way])
        half = spans(unit)[axis]
        recv((unit, 0, axis, way), w.at[(*at, half[0])])
        part = w.at[(*at, half[1 + way])]
        send((name, 0), (unit, 1, axis), part, part, devices[axis][way])

    crossed = ((x, xm, xp, x2), (z, zm, zp, z2))

    def far_at(axis, place, i):
        return (place, crossed[0][i]) if axis == 0 else (crossed[1][i], place)

    def far_own(unit, axis, i):
        w, name = buffers[unit], WEIGHT_OF[unit]
        half = spans(unit)[axis][0]
        block = w.at[(*far_at(axis, (z, x)[axis], i), half)]
        if i == 3:
            recv((unit, 1, axis), block)
        for way in range(2):
            send((name, 1), (unit, 2, axis, way, i), block, block, devices[1 - axis][way])

    def far_forward(unit, axis, way, i):
        w, name = buffers[unit], WEIGHT_OF[unit]
        at = far_at(axis, near[1 - axis][way], i)
        half = spans(unit)[axis]
        recv((unit, 2, axis, way, i), w.at[(*at, half[0])])
        part = w.at[(*at, half[1 + way])]
        send((name, 1), (unit, 3), part, part, devices[1 - axis][way])

    def weight_done(unit):
        first, a, _, b, _ = UNITS[unit]
        recv((unit, 3), buffers[unit].at[0, :, pl.ds(first, a + b)])

    mixer_bufs = (part1, pair1, sums1, ends1, relay1)
    ffn_bufs = (
        (part2, pair2, sums2, ends2, relay2),
        (part3, pair3, sums3, ends3, relay3),
    )

    def sum_pair(bufs, tag, ch):
        part, pair = bufs[:2]
        rows, _, _ = rows_of(ch)
        send((tag, 1), (tag, 0, ch), part.at[oc, :, rows], pair.at[:, rows], to_pt)

    def sum_start(bufs, tag, ch):
        part, pair, sums, ends, relay = bufs
        rows, low, high = rows_of(ch)
        half = pl.ds(128 * ch, 128)
        recv((tag, 0, ch), pair.at[:, rows])
        for place in (y2, yp, ym):
            sums[place, rows] = (
                part[c, place, rows].astype(F32) + pair[place, rows].astype(F32)
            ).astype(BF16)
        send((tag, 0), (tag, 1, ch), sums.at[y2, low], relay.at[0, half], to_yp)
        send((tag, 0), (tag, 2, ch), sums.at[y2, high], relay.at[1, half], to_ym)
        send((tag, 0), (tag, 3, ch), sums.at[yp, high], ends.at[1, high], to_yp)
        send((tag, 0), (tag, 3, ch), sums.at[ym, low], ends.at[0, low], to_ym)

    def sum_relay(bufs, tag, ch, side):
        _, _, sums, ends, relay = bufs
        _, low, high = rows_of(ch)
        half = pl.ds(128 * ch, 128)
        place, part, device = ((yp, low, to_yp), (ym, high, to_ym))[side]
        recv((tag, 1 + side, ch), relay.at[side, half])
        sums[place, part] = (
            sums[place, part].astype(F32) + relay[side, half].astype(F32)
        ).astype(BF16)
        send((tag, 0), (tag, 3, ch), sums.at[place, part], ends.at[1 - side, part], device)

    def sum_end(bufs, tag, ch):
        part, pair, _, ends, _ = bufs
        rows, _, _ = rows_of(ch)
        recv((tag, 3, ch), ends.at[:, rows])
        return (part[c, y, rows].astype(F32) + pair[y, rows].astype(F32)) + (
            ends[0, rows].astype(F32) + ends[1, rows].astype(F32)
        )

    stores = []

    def mixer_end(ch):
        rows, _, _ = rows_of(ch)
        total = sum_end(mixer_bufs, 12, ch)
        resid[y, c, rows] = (tok[y, c, rows].astype(F32) + total).astype(BF16)

    def ffn_end(ch, half):
        rows, _, _ = rows_of(ch)
        total = sum_end(ffn_bufs[half], 13 + half, ch)
        if half == 0:
            first[rows] = total
            return
        total = jnp.concatenate(
            [first[rows, :64], total[:, :64], first[rows, 64:], total[:, 64:]], axis=1
        )
        out_ref[rows, :] = (resid[y, c, rows].astype(F32) + total).astype(BF16)

    def norm_rows(buf, gain, ch):
        def body(i, carry):
            rows = pl.ds(pl.multiple_of(SEQ * ch + 32 * i, 32), 32)
            squares = None
            for p in range(8):
                block = buf[p // 2, p % 2, rows].astype(F32)
                squares = block * block if p == 0 else squares + block * block
            mean = jnp.sum(squares, axis=-1, keepdims=True) * (1.0 / 2048.0)
            factor = lax.rsqrt(mean + EPS)
            for p in range(8):
                lanes = slice(256 * p, 256 * p + 256)
                block = buf[p // 2, p % 2, rows].astype(F32)
                normed[rows, lanes] = (block * factor * gain[:, lanes]).astype(BF16)
            return carry

        lax.fori_loop(0, 8, body, 0, unroll=4)

    def mixer(ch):
        rows, _, _ = rows_of(ch)
        qkv = dot(normed[rows, :], w_qo[:, :, :, 0:256].reshape(2048, 256))
        gate = dot(normed[rows, :], w_qo[:, :, :, 256:384].reshape(2048, 128))
        gate = gate.astype(BF16).astype(F32)
        qk = qkv[:, :128].astype(BF16).astype(F32)
        value = qkv[:, 128:].astype(BF16)
        lane = lax.broadcasted_iota(jnp.int32, (SEQ, 128), 1)
        turned = jnp.where(
            lax.rem(lane, 2) == 0, pltpu.roll(qk, 127, axis=1), pltpu.roll(qk, 1, axis=1)
        )
        rotated = qk * cos_ref[...] + turned * sin_ref[...]
        queries = jnp.where(lane < DK, rotated, 0.0).astype(BF16)
        keys = pltpu.roll(rotated, DK, axis=1).astype(BF16)
        scores = lax.dot_general(
            queries, keys, (((1,), (1,)), ((), ())), preferred_element_type=F32
        )
        retained = dot((scores * mask[...]).astype(BF16), value)
        center = jnp.mean(retained, axis=-1, keepdims=True)
        moved = retained - center
        spread = jnp.mean(moved * moved, axis=-1, keepdims=True)
        grouped = moved * lax.rsqrt(spread + EPS) * head_gain[...]
        mixed[rows] = (grouped * silu(gate)).astype(BF16)

    def mixer_out(ch):
        rows, _, _ = rows_of(ch)

        def body(p, carry):
            py, pc = lax.div(p, 2), lax.rem(p, 2)
            block = jnp.concatenate(
                [w_qo[py, 2 * pc, :, 384:512], w_qo[py, 2 * pc + 1, :, 384:512]], axis=1
            )
            part1[pc, py, rows] = dot(mixed[rows], block).astype(BF16)
            return carry

        lax.fori_loop(0, 8, body, 0, unroll=True)

    def gate_up(ch, first):
        rows, _, _ = rows_of(ch)

        def body(j, carry):
            columns = pl.ds(pl.multiple_of(256 * j, 256), 256)
            both = dot(normed[rows, :], w_gu[:, :, :, columns].reshape(2048, 256))
            hidden[rows, pl.ds(pl.multiple_of(128 * j, 128), 128)] = (
                silu(both[:, :128]) * both[:, 128:]
            ).astype(BF16)
            return carry

        if first:
            lax.fori_loop(0, 3, body, 0, unroll=True)
            return
        lax.fori_loop(3, 5, body, 0, unroll=True)
        both = dot(normed[rows, :], w_gu[:, :, :, 1280:1408].reshape(2048, 128))
        hidden[rows, 640:768] = (silu(both) * pltpu.roll(both, 64, axis=1)).astype(BF16)

    def join(half):
        w = (w_d0, w_d1)[half]
        for py in range(4):
            top, low = [], []
            for k in range(4):
                block = w[py, k]
                top.append(block[:, :64])
                low.append(block[:, 64:])
            joined[half, py, 0:352, :] = jnp.concatenate(top, axis=1)
            joined[half, py, 352:704, :] = jnp.concatenate(low, axis=1)

    def down(ch, half):
        rows, _, _ = rows_of(ch)
        target = (part2, part3)[half]
        for py in range(4):
            both = dot(hidden[rows, :704], joined[half, py]).astype(BF16)
            target[0, py, rows] = both[:, :128]
            target[1, py, rows] = both[:, 128:]

    part = functools.partial
    actions = [part(near_own, axis=axis) for axis in range(2)]
    actions += [part(near_forward, axis=k // 2, way=k % 2) for k in range(4)]
    actions += [part(far_own, axis=k // 4, i=k % 4) for k in range(8)]
    actions += [part(far_forward, axis=k // 8, way=k // 4 % 2, i=k % 4) for k in range(16)]
    actions += [weight_done, stage_gate_up, stage_down, stage_rest]
    for tag, buf in ((10, tok), (11, resid)):
        actions.append(part(gather_own, buf, tag))
        actions += [part(gather_forward, buf, tag, side=side) for side in range(2)]
        actions += [part(gather_far, buf, tag), part(gather_done, buf, tag)]
    for tag, bufs, end in (
        (12, mixer_bufs, mixer_end),
        (13, ffn_bufs[0], part(ffn_end, half=0)),
        (14, ffn_bufs[1], part(ffn_end, half=1)),
    ):
        actions += [part(sum_pair, bufs, tag), part(sum_start, bufs, tag)]
        actions += [part(sum_relay, bufs, tag, side=side) for side in range(2)]
        actions.append(end)
    actions += [part(norm_rows, tok, mix_gain), mixer, mixer_out]
    actions += [part(norm_rows, resid, ffn_gain)]
    actions += [part(gate_up, first=True), part(gate_up, first=False)]
    actions += [part(down, half=0), part(down, half=1), join]
    for code in SCHEDULE:
        actions[code // 8](code % 8)

    for name, w in enumerate((w_qo, w_gu, w_d0, w_d1)):
        all_sent((name, 0), w.at[0, pl.ds(0, 3)])
        all_sent((name, 1), w.at[pl.ds(0, 3)])
    for tag, buf in ((10, tok), (11, resid)):
        all_sent((tag, 0), buf.at[pl.ds(0, 3), 0])
        all_sent((tag, 1), buf.at[:, 0])
    for tag, bufs in ((12, mixer_bufs), (13, ffn_bufs[0]), (14, ffn_bufs[1])):
        all_sent((tag, 0), bufs[2].at[pl.ds(0, 3)])
        all_sent((tag, 1), bufs[0].at[0])
    for copy in stores:
        copy.wait()
    assert len(ids) == RECEIVES and len(groups) == SENDS


def per_device(*args):
    (tokens, mix_gain, query_w, key_w, value_w, gate_w, out_w, head_gain, ffn_gain) = args[:9]
    ffn_gate, ffn_up, ffn_down = args[9:]
    cosine, sine = rope_tables()
    hbm = pl.BlockSpec(memory_space=pltpu.HBM)
    rows = tokens.shape[0]

    def sum_buffers(width):
        return [
            pltpu.VMEM((2, 4, rows, width), BF16),
            pltpu.VMEM((4, rows, width), BF16),
            pltpu.VMEM((4, rows, width), BF16),
            pltpu.VMEM((2, rows, width), BF16),
            pltpu.VMEM((2, rows // 2, width), BF16),
        ]

    call = pl.pallas_call(
        layer_kernel,
        out_shape=pltpu.VMEM((rows, 256), BF16),
        in_specs=[hbm] * 15,
        out_specs=pl.BlockSpec(memory_space=pltpu.VMEM),
        scratch_shapes=[
            pltpu.VMEM((4, 2, rows, 256), BF16),
            pltpu.VMEM((4, 2, rows, 256), BF16),
            pltpu.VMEM((rows, 2048), BF16),
            pltpu.VMEM((4, 4, 128, 512), BF16),
            pltpu.VMEM((4, 4, 128, 1408), BF16),
            pltpu.VMEM((4, 4, 352, 128), BF16),
            pltpu.VMEM((4, 4, 352, 128), BF16),
            pltpu.VMEM((2, 4, 704, 256), BF16),
            pltpu.VMEM((704, 128), BF16),
            pltpu.VMEM((2 * DK, 128), BF16),
            pltpu.VMEM((1408, 128), BF16),
            pltpu.VMEM((1, 2048), F32),
            pltpu.VMEM((1, 2048), F32),
            pltpu.VMEM((1, DV), F32),
            pltpu.VMEM((SEQ, 128), F32),
            pltpu.VMEM((SEQ, 128), F32),
            pltpu.VMEM((HEADS, 8, 128), F32),
            pltpu.VMEM((SEQ, SEQ), F32),
            pltpu.VMEM((rows, DV), BF16),
            pltpu.VMEM((rows, 768), BF16),
            *sum_buffers(256),
            *sum_buffers(128),
            *sum_buffers(128),
            pltpu.VMEM((rows, 128), F32),
            pltpu.SemaphoreType.DMA((32,)),
            pltpu.SemaphoreType.DMA((SENDS,)),
            pltpu.SemaphoreType.DMA((RECEIVES,)),
        ],
        compiler_params=pltpu.CompilerParams(
            collective_id=0, has_side_effects=True, vmem_limit_bytes=54 * 2**20
        ),
        cost_estimate=pl.CostEstimate(
            flops=11_000_000_000, bytes_accessed=4_000_000, transcendentals=1_000_000
        ),
        name="layer",
    )
    return call(
        tokens,
        mix_gain.reshape(1, -1),
        query_w.T,
        key_w.T,
        value_w,
        gate_w,
        out_w,
        head_gain,
        ffn_gain.reshape(1, -1),
        ffn_gate.T,
        ffn_up.T,
        ffn_down,
        jnp.asarray(cosine),
        jnp.asarray(sine),
        jnp.asarray(decay_table()),
    )


def solution(mesh):
    placed = (
        P(("rep", "fs"), "tp"),
        P(),
        P("fs", "tp"),
        P("fs", "tp"),
        P("fs", "tp"),
        P("fs", "tp"),
        P("tp", "fs"),
        P("tp", None),
        P(),
        P("fs", "tp"),
        P("fs", "tp"),
        P("tp", "fs"),
    )
    return jax.shard_map(
        per_device, mesh=mesh, in_specs=placed, out_specs=P(("rep", "fs"), "tp"), check_vma=False
    )
```

```python
import functools

import jax
import jax.numpy as jnp
import numpy as np
from jax import lax
from jax.experimental import pallas as pl
from jax.experimental.pallas import tpu as pltpu
from jax.sharding import PartitionSpec as P

HEADS = 8
DK = 64
DV = 128
SEQ = 256
EPS = 1e-06
ROPE_BASE = 10000.0
F32 = jnp.float32
BF16 = jnp.bfloat16
MESH = pl.DeviceIdType.MESH
RECEIVES = 195
SENDS = 18

UNITS = (
    (0, 64, 32, 64, 32),
    (0, 32, 16, 32, 16),
    (64, 32, 16, 32, 16),
    (0, 176, 96, 176, 96),
    (0, 176, 96, 176, 96),
)
WEIGHT_OF = (0, 1, 1, 2, 3)

SCHEDULE = (
    0, 8, 274, 272, 80, 248, 48, 9, 2, 16, 24, 40, 32, 273, 96, 264,
    64, 56, 144, 176, 208, 282, 88, 290, 112, 288, 72, 104, 1, 280, 275, 10,
    128, 289, 160, 192, 120, 184, 224, 216, 256, 298, 152, 168, 136, 232, 200, 11,
    296, 81, 306, 281, 49, 33, 474, 41, 17, 25, 97, 57, 304, 65, 3, 472,
    89, 283, 291, 240, 480, 488, 352, 297, 482, 490, 299, 105, 73, 177, 354, 360,
    305, 473, 481, 307, 225, 121, 145, 489, 362, 209, 153, 113, 185, 217, 129, 193,
    161, 353, 475, 483, 233, 169, 137, 201, 376, 368, 491, 34, 12, 35, 42, 19,
    26, 361, 4, 18, 27, 370, 378, 43, 52, 82, 51, 241, 83, 59, 384, 312,
    50, 98, 99, 106, 377, 74, 355, 58, 90, 369, 210, 36, 44, 386, 66, 314,
    67, 91, 20, 363, 75, 328, 28, 100, 385, 320, 107, 170, 138, 154, 178, 322,
    218, 122, 146, 202, 226, 330, 194, 114, 162, 379, 371, 313, 130, 186, 234, 147,
    84, 60, 92, 123, 68, 76, 219, 108, 187, 336, 195, 115, 179, 171, 163, 148,
    211, 203, 139, 196, 338, 235, 344, 228, 155, 131, 116, 227, 496, 387, 315, 242,
    346, 498, 506, 156, 124, 220, 180, 504, 321, 329, 188, 132, 212, 204, 236, 172,
    164, 140, 514, 512, 243, 536, 522, 394, 331, 323, 520, 392, 244, 337, 537, 402,
    530, 434, 528, 400, 345, 432, 497, 505, 339, 442, 513, 440, 521, 418, 393, 410,
    347, 529, 499, 416, 408, 507, 401, 433, 515, 450, 458, 523, 395, 456, 448, 531,
    435, 441, 426, 424, 403, 443, 466, 409, 417, 464, 457, 449, 411, 419, 451, 459,
    425, 465, 427, 467,
)


def rope_tables():
    half = DK // 2
    frequency = ROPE_BASE ** (-np.linspace(0.0, 1.0, half))
    angles = np.arange(SEQ)[:, None] * frequency[None, :]
    cosine = np.repeat(np.cos(angles), 2, axis=1)
    sine = np.repeat(np.sin(angles), 2, axis=1) * np.tile([-1.0, 1.0], half)
    scale = DK**-0.5
    return (
        np.concatenate([cosine, cosine * scale], axis=1).astype(np.float32),
        np.concatenate([sine, sine * scale], axis=1).astype(np.float32),
    )


def decay_table():
    rates = np.log1p(-np.exp2(-5.0 - 4.0 * np.arange(HEADS) / (HEADS - 1)))
    return np.broadcast_to(rates[:, None, None], (HEADS, 8, 128)).astype(np.float32)


def silu(values):
    return values / (1.0 + jnp.exp(-values))


def dot(left, right):
    return jnp.dot(left, right, preferred_element_type=F32)


def layer_kernel(
    tok_hbm,
    mix_gain_hbm,
    query_hbm,
    key_hbm,
    value_hbm,
    gate_hbm,
    out_w_hbm,
    head_gain_hbm,
    ffn_gain_hbm,
    ffn_gate_hbm,
    ffn_up_hbm,
    down_hbm,
    cos_hbm,
    sin_hbm,
    rate_hbm,
    out_ref,
    tok,
    resid,
    normed,
    w_qo,
    w_gu,
    w_d0,
    w_d1,
    joined,
    down_in,
    turn_qk,
    turn_gu,
    mix_gain,
    ffn_gain,
    head_gain,
    cos_ref,
    sin_ref,
    rate_ref,
    mask,
    mixed,
    hidden,
    part1,
    pair1,
    sums1,
    ends1,
    relay1,
    part2,
    pair2,
    sums2,
    ends2,
    relay2,
    part3,
    pair3,
    sums3,
    ends3,
    relay3,
    first,
    local_sem,
    send_sem,
    recv_sem,
):
    rep, fs, tp = lax.axis_index("rep"), lax.axis_index("fs"), lax.axis_index("tp")
    y, c = lax.div(tp, 2), lax.rem(tp, 2)
    z, x = lax.div(fs, 4), lax.rem(fs, 4)
    oc = 1 - c

    def step(value, by, size):
        return lax.rem(value + by, size)

    yp, y2, ym = step(y, 1, 4), step(y, 2, 4), step(y, 3, 4)
    xp, x2, xm = step(x, 1, 4), step(x, 2, 4), step(x, 3, 4)
    zp, z2, zm = step(z, 1, 4), step(z, 2, 4), step(z, 3, 4)
    zall = rep * 4 + z

    def z_device(place):
        return (lax.div(place, 4), lax.rem(place, 4) * 4 + x, tp)

    to_yp, to_ym = (rep, fs, yp * 2 + c), (rep, fs, ym * 2 + c)
    to_pt = (rep, fs, y * 2 + oc)
    to_xp, to_xm = (rep, z * 4 + xp, tp), (rep, z * 4 + xm, tp)
    to_zp, to_zm = z_device(step(zall, 1, 8)), z_device(step(zall, 7, 8))

    barrier = pltpu.get_barrier_semaphore()
    peers = (to_yp, to_ym, to_pt, to_xp, to_xm, to_zp, to_zm)
    for peer in peers:
        pl.semaphore_signal(barrier, inc=1, device_id=peer, device_id_type=MESH)

    ids = {}
    groups = {}

    def send(group, key, src, dst, device):
        k = ids.setdefault(key, len(ids))
        g = groups.setdefault(group, len(groups))
        pltpu.make_async_remote_copy(
            src_ref=src,
            dst_ref=dst,
            send_sem=send_sem.at[g],
            recv_sem=recv_sem.at[k],
            device_id=device,
            device_id_type=MESH,
        ).start()

    def recv(key, dst):
        pltpu.make_async_remote_copy(
            src_ref=dst,
            dst_ref=dst,
            send_sem=send_sem.at[0],
            recv_sem=recv_sem.at[ids[key]],
            device_id=to_pt,
            device_id_type=MESH,
        ).wait_recv()

    def all_sent(group, src):
        pltpu.make_async_remote_copy(
            src_ref=src,
            dst_ref=src,
            send_sem=send_sem.at[groups[group]],
            recv_sem=recv_sem.at[0],
            device_id=to_pt,
            device_id_type=MESH,
        ).wait_send()

    count = [0]

    def local(src, dst):
        copy = pltpu.make_async_copy(src, dst, local_sem.at[count[0]])
        count[0] += 1
        copy.start()
        return copy

    load_qk = [
        local(query_hbm, turn_qk.at[pl.ds(0, DK)]),
        local(key_hbm, turn_qk.at[pl.ds(DK, DK)]),
    ]
    load_vgo = [
        local(value_hbm, w_qo.at[z, x, :, pl.ds(128, 128)]),
        local(gate_hbm, w_qo.at[z, x, :, pl.ds(256, 128)]),
        local(out_w_hbm, w_qo.at[z, x, :, pl.ds(384, 128)]),
    ]
    load_tok = [local(tok_hbm, tok.at[y, c])]
    load_gu = []
    for j in range(6):
        width = 128 if j < 5 else 64
        for k, source in enumerate((ffn_gate_hbm, ffn_up_hbm)):
            place = pl.ds(256 * j + width * k, width)
            load_gu.append(local(source.at[pl.ds(128 * j, width)], turn_gu.at[place]))
    load_down = [local(down_hbm, down_in)]
    load_rest = [
        local(mix_gain_hbm, mix_gain),
        local(ffn_gain_hbm, ffn_gain),
        local(head_gain_hbm, head_gain),
        local(cos_hbm, cos_ref),
        local(sin_hbm, sin_ref),
        local(rate_hbm, rate_ref),
    ]

    def loaded(copies):
        for copy in copies:
            copy.wait()

    loaded(load_qk)
    w_qo[z, x, :, 0:128] = turn_qk[...].T
    loaded(load_vgo)
    loaded(load_tok)
    pl.semaphore_wait(barrier, len(peers))

    def stage_gate_up(_):
        loaded(load_gu)
        for j in range(11):
            lanes = slice(128 * j, 128 * j + 128)
            w_gu[z, x, :, lanes] = turn_gu[lanes, :].T

    def stage_down(_):
        loaded(load_down)
        top, low = down_in[0:352, :], down_in[352:704, :]
        w_d0[z, x] = jnp.concatenate([top[:, :64], low[:, :64]], axis=1)
        w_d1[z, x] = jnp.concatenate([top[:, 64:], low[:, 64:]], axis=1)

    def stage_rest(_):
        loaded(load_rest)
        gap = lax.broadcasted_iota(jnp.int32, (SEQ, 128), 0) - lax.broadcasted_iota(
            jnp.int32, (SEQ, 128), 1
        )
        rate = rate_ref[tp][:1, :]
        for half in range(2):
            distance = (gap - 128 * half).astype(F32)
            mask[:, 128 * half : 128 * half + 128] = jnp.where(
                distance >= 0.0, jnp.exp(jnp.maximum(distance, 0.0) * rate), 0.0
            )

    def rows_of(ch):
        return pl.ds(SEQ * ch, SEQ), pl.ds(SEQ * ch, 128), pl.ds(SEQ * ch + 128, 128)

    def gather_own(buf, tag, ch):
        rows, _, _ = rows_of(ch)
        own = buf.at[y, c, rows]
        send((tag, 0), (tag, 0, ch), own, own, to_yp)
        send((tag, 0), (tag, 1, ch), own, own, to_ym)
        send((tag, 1), (tag, 3, ch), own, own, to_pt)

    def gather_forward(buf, tag, ch, side):
        rows, low, high = rows_of(ch)
        row, part, device = ((ym, low, to_yp), (yp, high, to_ym))[side]
        recv((tag, side, ch), buf.at[row, c, rows])
        send((tag, 0), (tag, 2, ch), buf.at[row, c, part], buf.at[row, c, part], device)
        send((tag, 1), (tag, 3, ch), buf.at[row, c, rows], buf.at[row, c, rows], to_pt)

    def gather_far(buf, tag, ch):
        rows, _, _ = rows_of(ch)
        recv((tag, 2, ch), buf.at[y2, c, rows])
        send((tag, 1), (tag, 3, ch), buf.at[y2, c, rows], buf.at[y2, c, rows], to_pt)

    def gather_done(buf, tag, ch):
        rows, _, _ = rows_of(ch)
        recv((tag, 3, ch), buf.at[:, oc, rows])

    buffers = (w_qo, w_gu, w_gu, w_d0, w_d1)

    def spans(unit):
        first, a, a0, b, b0 = UNITS[unit]
        half_a = (pl.ds(first, a), pl.ds(first, a0), pl.ds(first + a0, a - a0))
        first = first + a
        return half_a, (pl.ds(first, b), pl.ds(first, b0), pl.ds(first + b0, b - b0))

    near = ((xm, xp), (zm, zp))
    far = (x2, z2)
    devices = ((to_xp, to_xm), (to_zp, to_zm))

    def near_at(axis, place):
        return (z, place) if axis == 0 else (place, x)

    def near_own(unit, axis):
        w, name = buffers[unit], WEIGHT_OF[unit]
        half = spans(unit)[axis][0]
        own = w.at[z, x, half]
        for way in range(2):
            send((name, 0), (unit, 0, axis, way), own, own, devices[axis][way])

    def near_forward(unit, axis, way):
        w, name = buffers[unit], WEIGHT_OF[unit]
        at = near_at(axis, near[axis][way])
        half = spans(unit)[axis]
        recv((unit, 0, axis, way), w.at[(*at, half[0])])
        part = w.at[(*at, half[1 + way])]
        send((name, 0), (unit, 1, axis), part, part, devices[axis][way])

    crossed = ((x, xm, xp, x2), (z, zm, zp, z2))

    def far_at(axis, place, i):
        return (place, crossed[0][i]) if axis == 0 else (crossed[1][i], place)

    def far_own(unit, axis, i):
        w, name = buffers[unit], WEIGHT_OF[unit]
        half = spans(unit)[axis][0]
        block = w.at[(*far_at(axis, (z, x)[axis], i), half)]
        if i == 3:
            recv((unit, 1, axis), block)
        for way in range(2):
            send((name, 1), (unit, 2, axis, way, i), block, block, devices[1 - axis][way])

    def far_forward(unit, axis, way, i):
        w, name = buffers[unit], WEIGHT_OF[unit]
        at = far_at(axis, near[1 - axis][way], i)
        half = spans(unit)[axis]
        recv((unit, 2, axis, way, i), w.at[(*at, half[0])])
        part = w.at[(*at, half[1 + way])]
        send((name, 1), (unit, 3), part, part, devices[1 - axis][way])

    def weight_done(unit):
        first, a, _, b, _ = UNITS[unit]
        recv((unit, 3), buffers[unit].at[0, :, pl.ds(first, a + b)])

    mixer_bufs = (part1, pair1, sums1, ends1, relay1)
    ffn_bufs = (
        (part2, pair2, sums2, ends2, relay2),
        (part3, pair3, sums3, ends3, relay3),
    )

    def sum_pair(bufs, tag, ch):
        part, pair = bufs[:2]
        rows, _, _ = rows_of(ch)
        send((tag, 1), (tag, 0, ch), part.at[oc, :, rows], pair.at[:, rows], to_pt)

    def sum_start(bufs, tag, ch):
        part, pair, sums, ends, relay = bufs
        rows, low, high = rows_of(ch)
        half = pl.ds(128 * ch, 128)
        recv((tag, 0, ch), pair.at[:, rows])
        for place in (y2, yp, ym):
            sums[place, rows] = (
                part[c, place, rows].astype(F32) + pair[place, rows].astype(F32)
            ).astype(BF16)
        send((tag, 0), (tag, 1, ch), sums.at[y2, low], relay.at[0, half], to_yp)
        send((tag, 0), (tag, 2, ch), sums.at[y2, high], relay.at[1, half], to_ym)
        send((tag, 0), (tag, 3, ch), sums.at[yp, high], ends.at[1, high], to_yp)
        send((tag, 0), (tag, 3, ch), sums.at[ym, low], ends.at[0, low], to_ym)

    def sum_relay(bufs, tag, ch, side):
        _, _, sums, ends, relay = bufs
        _, low, high = rows_of(ch)
        half = pl.ds(128 * ch, 128)
        place, part, device = ((yp, low, to_yp), (ym, high, to_ym))[side]
        recv((tag, 1 + side, ch), relay.at[side, half])
        sums[place, part] = (
            sums[place, part].astype(F32) + relay[side, half].astype(F32)
        ).astype(BF16)
        send((tag, 0), (tag, 3, ch), sums.at[place, part], ends.at[1 - side, part], device)

    def sum_end(bufs, tag, ch):
        part, pair, _, ends, _ = bufs
        rows, _, _ = rows_of(ch)
        recv((tag, 3, ch), ends.at[:, rows])
        return (part[c, y, rows].astype(F32) + pair[y, rows].astype(F32)) + (
            ends[0, rows].astype(F32) + ends[1, rows].astype(F32)
        )

    def mixer_end(ch):
        rows, _, _ = rows_of(ch)
        total = sum_end(mixer_bufs, 12, ch)
        resid[y, c, rows] = (tok[y, c, rows].astype(F32) + total).astype(BF16)

    def ffn_end(ch, half):
        rows, _, _ = rows_of(ch)
        total = sum_end(ffn_bufs[half], 13 + half, ch)
        if half == 0:
            first[rows] = total
            return
        total = jnp.concatenate(
            [first[rows, :64], total[:, :64], first[rows, 64:], total[:, 64:]], axis=1
        )
        out_ref[rows, :] = (resid[y, c, rows].astype(F32) + total).astype(BF16)

    def norm_rows(buf, gain, ch):
        def body(i, carry):
            rows = pl.ds(pl.multiple_of(SEQ * ch + 32 * i, 32), 32)
            squares = None
            for p in range(8):
                block = buf[p // 2, p % 2, rows].astype(F32)
                squares = block * block if p == 0 else squares + block * block
            mean = jnp.sum(squares, axis=-1, keepdims=True) * (1.0 / 2048.0)
            factor = lax.rsqrt(mean + EPS)
            for p in range(8):
                lanes = slice(256 * p, 256 * p + 256)
                block = buf[p // 2, p % 2, rows].astype(F32)
                normed[rows, lanes] = (block * factor * gain[:, lanes]).astype(BF16)
            return carry

        lax.fori_loop(0, 8, body, 0, unroll=4)

    def mixer(ch):
        rows, _, _ = rows_of(ch)
        qkv = dot(normed[rows, :], w_qo[:, :, :, 0:256].reshape(2048, 256))
        gate = dot(normed[rows, :], w_qo[:, :, :, 256:384].reshape(2048, 128))
        gate = gate.astype(BF16).astype(F32)
        qk = qkv[:, :128].astype(BF16).astype(F32)
        value = qkv[:, 128:].astype(BF16)
        lane = lax.broadcasted_iota(jnp.int32, (SEQ, 128), 1)
        turned = jnp.where(
            lax.rem(lane, 2) == 0, pltpu.roll(qk, 127, axis=1), pltpu.roll(qk, 1, axis=1)
        )
        rotated = qk * cos_ref[...] + turned * sin_ref[...]
        queries = jnp.where(lane < DK, rotated, 0.0).astype(BF16)
        keys = pltpu.roll(rotated, DK, axis=1).astype(BF16)
        scores = lax.dot_general(
            queries, keys, (((1,), (1,)), ((), ())), preferred_element_type=F32
        )
        retained = dot((scores * mask[...]).astype(BF16), value)
        center = jnp.mean(retained, axis=-1, keepdims=True)
        moved = retained - center
        spread = jnp.mean(moved * moved, axis=-1, keepdims=True)
        grouped = moved * lax.rsqrt(spread + EPS) * head_gain[...]
        mixed[rows] = (grouped * silu(gate)).astype(BF16)

    def mixer_out(ch):
        rows, _, _ = rows_of(ch)

        def body(p, carry):
            py, pc = lax.div(p, 2), lax.rem(p, 2)
            block = jnp.concatenate(
                [w_qo[py, 2 * pc, :, 384:512], w_qo[py, 2 * pc + 1, :, 384:512]], axis=1
            )
            part1[pc, py, rows] = dot(mixed[rows], block).astype(BF16)
            return carry

        lax.fori_loop(0, 8, body, 0, unroll=True)

    def gate_up(ch, first):
        rows, _, _ = rows_of(ch)

        def body(j, carry):
            columns = pl.ds(pl.multiple_of(256 * j, 256), 256)
            both = dot(normed[rows, :], w_gu[:, :, :, columns].reshape(2048, 256))
            hidden[rows, pl.ds(pl.multiple_of(128 * j, 128), 128)] = (
                silu(both[:, :128]) * both[:, 128:]
            ).astype(BF16)
            return carry

        if first:
            lax.fori_loop(0, 3, body, 0, unroll=True)
            return
        lax.fori_loop(3, 5, body, 0, unroll=True)
        both = dot(normed[rows, :], w_gu[:, :, :, 1280:1408].reshape(2048, 128))
        hidden[rows, 640:768] = (silu(both) * pltpu.roll(both, 64, axis=1)).astype(BF16)

    def join(half):
        w = (w_d0, w_d1)[half]
        for py in range(4):
            top, low = [], []
            for k in range(4):
                block = w[py, k]
                top.append(block[:, :64])
                low.append(block[:, 64:])
            joined[half, py, 0:352, :] = jnp.concatenate(top, axis=1)
            joined[half, py, 352:704, :] = jnp.concatenate(low, axis=1)

    def down(ch, half):
        rows, _, _ = rows_of(ch)
        target = (part2, part3)[half]
        for py in range(4):
            both = dot(hidden[rows, :704], joined[half, py]).astype(BF16)
            target[0, py, rows] = both[:, :128]
            target[1, py, rows] = both[:, 128:]

    part = functools.partial
    actions = [part(near_own, axis=axis) for axis in range(2)]
    actions += [part(near_forward, axis=k // 2, way=k % 2) for k in range(4)]
    actions += [part(far_own, axis=k // 4, i=k % 4) for k in range(8)]
    actions += [part(far_forward, axis=k // 8, way=k // 4 % 2, i=k % 4) for k in range(16)]
    actions += [weight_done, stage_gate_up, stage_down, stage_rest]
    for tag, buf in ((10, tok), (11, resid)):
        actions.append(part(gather_own, buf, tag))
        actions += [part(gather_forward, buf, tag, side=side) for side in range(2)]
        actions += [part(gather_far, buf, tag), part(gather_done, buf, tag)]
    for tag, bufs, end in (
        (12, mixer_bufs, mixer_end),
        (13, ffn_bufs[0], part(ffn_end, half=0)),
        (14, ffn_bufs[1], part(ffn_end, half=1)),
    ):
        actions += [part(sum_pair, bufs, tag), part(sum_start, bufs, tag)]
        actions += [part(sum_relay, bufs, tag, side=side) for side in range(2)]
        actions.append(end)
    actions += [part(norm_rows, tok, mix_gain), mixer, mixer_out]
    actions += [part(norm_rows, resid, ffn_gain)]
    actions += [part(gate_up, first=True), part(gate_up, first=False)]
    actions += [part(down, half=0), part(down, half=1), join]
    for code in SCHEDULE:
        actions[code // 8](code % 8)

    for name, w in enumerate((w_qo, w_gu, w_d0, w_d1)):
        all_sent((name, 0), w.at[0, pl.ds(0, 3)])
        all_sent((name, 1), w.at[pl.ds(0, 3)])
    for tag, buf in ((10, tok), (11, resid)):
        all_sent((tag, 0), buf.at[pl.ds(0, 3), 0])
        all_sent((tag, 1), buf.at[:, 0])
    for tag, bufs in ((12, mixer_bufs), (13, ffn_bufs[0]), (14, ffn_bufs[1])):
        all_sent((tag, 0), bufs[2].at[pl.ds(0, 3)])
        all_sent((tag, 1), bufs[0].at[0])
    assert len(ids) == RECEIVES and len(groups) == SENDS


def per_device(*args):
    (tokens, mix_gain, query_w, key_w, value_w, gate_w, out_w, head_gain, ffn_gain) = args[:9]
    ffn_gate, ffn_up, ffn_down = args[9:]
    cosine, sine = rope_tables()
    hbm = pl.BlockSpec(memory_space=pltpu.HBM)
    rows = tokens.shape[0]

    def sum_buffers(width):
        return [
            pltpu.VMEM((2, 4, rows, width), BF16),
            pltpu.VMEM((4, rows, width), BF16),
            pltpu.VMEM((4, rows, width), BF16),
            pltpu.VMEM((2, rows, width), BF16),
            pltpu.VMEM((2, rows // 2, width), BF16),
        ]

    call = pl.pallas_call(
        layer_kernel,
        out_shape=pltpu.VMEM((rows, 256), BF16),
        in_specs=[hbm] * 15,
        out_specs=pl.BlockSpec(memory_space=pltpu.VMEM),
        scratch_shapes=[
            pltpu.VMEM((4, 2, rows, 256), BF16),
            pltpu.VMEM((4, 2, rows, 256), BF16),
            pltpu.VMEM((rows, 2048), BF16),
            pltpu.VMEM((4, 4, 128, 512), BF16),
            pltpu.VMEM((4, 4, 128, 1408), BF16),
            pltpu.VMEM((4, 4, 352, 128), BF16),
            pltpu.VMEM((4, 4, 352, 128), BF16),
            pltpu.VMEM((2, 4, 704, 256), BF16),
            pltpu.VMEM((704, 128), BF16),
            pltpu.VMEM((2 * DK, 128), BF16),
            pltpu.VMEM((1408, 128), BF16),
            pltpu.VMEM((1, 2048), F32),
            pltpu.VMEM((1, 2048), F32),
            pltpu.VMEM((1, DV), F32),
            pltpu.VMEM((SEQ, 128), F32),
            pltpu.VMEM((SEQ, 128), F32),
            pltpu.VMEM((HEADS, 8, 128), F32),
            pltpu.VMEM((SEQ, SEQ), F32),
            pltpu.VMEM((rows, DV), BF16),
            pltpu.VMEM((rows, 768), BF16),
            *sum_buffers(256),
            *sum_buffers(128),
            *sum_buffers(128),
            pltpu.VMEM((rows, 128), F32),
            pltpu.SemaphoreType.DMA((32,)),
            pltpu.SemaphoreType.DMA((SENDS,)),
            pltpu.SemaphoreType.DMA((RECEIVES,)),
        ],
        compiler_params=pltpu.CompilerParams(
            collective_id=0, has_side_effects=True, vmem_limit_bytes=54 * 2**20
        ),
        cost_estimate=pl.CostEstimate(
            flops=11_000_000_000, bytes_accessed=4_000_000, transcendentals=1_000_000
        ),
        name="layer",
    )
    return call(
        tokens,
        mix_gain.reshape(1, -1),
        query_w.T,
        key_w.T,
        value_w,
        gate_w,
        out_w,
        head_gain,
        ffn_gain.reshape(1, -1),
        ffn_gate.T,
        ffn_up.T,
        ffn_down,
        jnp.asarray(cosine),
        jnp.asarray(sine),
        jnp.asarray(decay_table()),
    )


def solution(mesh):
    placed = (
        P(("rep", "fs"), "tp"),
        P(),
        P("fs", "tp"),
        P("fs", "tp"),
        P("fs", "tp"),
        P("fs", "tp"),
        P("tp", "fs"),
        P("tp", None),
        P(),
        P("fs", "tp"),
        P("fs", "tp"),
        P("tp", "fs"),
    )
    return jax.shard_map(
        per_device, mesh=mesh, in_specs=placed, out_specs=P(("rep", "fs"), "tp"), check_vma=False
    )
```

```python
import functools

import jax
import jax.numpy as jnp
import numpy as np
from jax import lax
from jax.experimental import pallas as pl
from jax.experimental.pallas import tpu as pltpu
from jax.sharding import PartitionSpec as P

HEADS = 8
DK = 64
DV = 128
SEQ = 256
EPS = 1e-06
ROPE_BASE = 10000.0
F32 = jnp.float32
BF16 = jnp.bfloat16
MESH = pl.DeviceIdType.MESH
RECEIVES = 195
SENDS = 18

UNITS = (
    (0, 64, 32, 64, 32),
    (0, 32, 16, 32, 16),
    (64, 32, 16, 32, 16),
    (0, 176, 96, 176, 96),
    (0, 176, 96, 176, 96),
)
WEIGHT_OF = (0, 1, 1, 2, 3)

SCHEDULE = (
    0, 8, 273, 272, 80, 264, 48, 248, 9, 1, 16, 24, 32, 40, 64, 88,
    289, 281, 56, 96, 275, 208, 176, 72, 104, 280, 144, 288, 112, 33, 184, 128,
    2, 41, 160, 216, 297, 274, 152, 305, 224, 120, 192, 168, 136, 200, 232, 49,
    25, 296, 291, 283, 256, 65, 105, 10, 17, 89, 97, 473, 57, 81, 304, 3,
    472, 282, 290, 240, 480, 488, 352, 299, 481, 489, 73, 201, 353, 360, 307, 298,
    475, 113, 161, 11, 145, 233, 129, 185, 483, 225, 306, 361, 491, 121, 153, 355,
    193, 217, 474, 209, 177, 137, 169, 50, 82, 368, 376, 482, 363, 490, 18, 34,
    27, 369, 42, 43, 19, 4, 59, 354, 90, 67, 12, 241, 26, 377, 384, 312,
    58, 98, 371, 35, 28, 106, 66, 99, 75, 379, 385, 313, 74, 178, 362, 20,
    107, 44, 91, 83, 218, 51, 36, 122, 84, 328, 320, 387, 60, 194, 210, 162,
    146, 321, 329, 202, 154, 130, 138, 226, 378, 234, 370, 186, 114, 170, 108, 92,
    211, 315, 195, 76, 68, 100, 52, 163, 115, 147, 336, 227, 179, 131, 219, 139,
    212, 187, 123, 156, 171, 203, 180, 337, 155, 344, 496, 235, 124, 386, 314, 242,
    345, 504, 140, 204, 497, 164, 220, 505, 323, 331, 132, 148, 188, 116, 236, 228,
    196, 172, 513, 512, 243, 536, 520, 392, 322, 330, 521, 393, 244, 339, 537, 400,
    529, 433, 528, 432, 347, 401, 499, 507, 338, 441, 515, 440, 523, 408, 395, 346,
    531, 498, 416, 409, 417, 506, 403, 435, 514, 457, 449, 522, 394, 456, 448, 443,
    530, 434, 424, 425, 402, 442, 465, 411, 464, 419, 451, 459, 410, 418, 450, 458,
    427, 467, 426, 466,
)


def rope_tables():
    half = DK // 2
    frequency = ROPE_BASE ** (-np.linspace(0.0, 1.0, half))
    angles = np.arange(SEQ)[:, None] * frequency[None, :]
    cosine = np.repeat(np.cos(angles), 2, axis=1)
    sine = np.repeat(np.sin(angles), 2, axis=1) * np.tile([-1.0, 1.0], half)
    scale = DK**-0.5
    return (
        np.concatenate([cosine, cosine * scale], axis=1).astype(np.float32),
        np.concatenate([sine, sine * scale], axis=1).astype(np.float32),
    )


def decay_table():
    rates = np.log1p(-np.exp2(-5.0 - 4.0 * np.arange(HEADS) / (HEADS - 1)))
    return np.broadcast_to(rates[:, None, None], (HEADS, 8, 128)).astype(np.float32)


def silu(values):
    return values / (1.0 + jnp.exp(-values))


def dot(left, right):
    return jnp.dot(left, right, preferred_element_type=F32)


def layer_kernel(
    tok_hbm,
    mix_gain_hbm,
    query_hbm,
    key_hbm,
    value_hbm,
    gate_hbm,
    out_w_hbm,
    head_gain_hbm,
    ffn_gain_hbm,
    ffn_gate_hbm,
    ffn_up_hbm,
    down_hbm,
    cos_hbm,
    sin_hbm,
    rate_hbm,
    out_ref,
    tok,
    resid,
    normed,
    w_qo,
    w_gu,
    w_d0,
    w_d1,
    joined,
    down_in,
    turn_qk,
    turn_gu,
    mix_gain,
    ffn_gain,
    head_gain,
    cos_ref,
    sin_ref,
    rate_ref,
    mask,
    mixed,
    hidden,
    part1,
    pair1,
    sums1,
    ends1,
    relay1,
    part2,
    pair2,
    sums2,
    ends2,
    relay2,
    part3,
    pair3,
    sums3,
    ends3,
    relay3,
    first,
    local_sem,
    send_sem,
    recv_sem,
):
    rep, fs, tp = lax.axis_index("rep"), lax.axis_index("fs"), lax.axis_index("tp")
    y, c = lax.div(tp, 2), lax.rem(tp, 2)
    z, x = lax.div(fs, 4), lax.rem(fs, 4)
    oc = 1 - c

    def step(value, by, size):
        return lax.rem(value + by, size)

    yp, y2, ym = step(y, 1, 4), step(y, 2, 4), step(y, 3, 4)
    xp, x2, xm = step(x, 1, 4), step(x, 2, 4), step(x, 3, 4)
    zp, z2, zm = step(z, 1, 4), step(z, 2, 4), step(z, 3, 4)
    zall = rep * 4 + z

    def z_device(place):
        return (lax.div(place, 4), lax.rem(place, 4) * 4 + x, tp)

    to_yp, to_ym = (rep, fs, yp * 2 + c), (rep, fs, ym * 2 + c)
    to_pt = (rep, fs, y * 2 + oc)
    to_xp, to_xm = (rep, z * 4 + xp, tp), (rep, z * 4 + xm, tp)
    to_zp, to_zm = z_device(step(zall, 1, 8)), z_device(step(zall, 7, 8))

    barrier = pltpu.get_barrier_semaphore()
    peers = (to_yp, to_ym, to_pt, to_xp, to_xm, to_zp, to_zm)
    for peer in peers:
        pl.semaphore_signal(barrier, inc=1, device_id=peer, device_id_type=MESH)

    ids = {}
    groups = {}

    def send(group, key, src, dst, device):
        k = ids.setdefault(key, len(ids))
        g = groups.setdefault(group, len(groups))
        pltpu.make_async_remote_copy(
            src_ref=src,
            dst_ref=dst,
            send_sem=send_sem.at[g],
            recv_sem=recv_sem.at[k],
            device_id=device,
            device_id_type=MESH,
        ).start()

    def recv(key, dst):
        pltpu.make_async_remote_copy(
            src_ref=dst,
            dst_ref=dst,
            send_sem=send_sem.at[0],
            recv_sem=recv_sem.at[ids[key]],
            device_id=to_pt,
            device_id_type=MESH,
        ).wait_recv()

    def all_sent(group, src):
        pltpu.make_async_remote_copy(
            src_ref=src,
            dst_ref=src,
            send_sem=send_sem.at[groups[group]],
            recv_sem=recv_sem.at[0],
            device_id=to_pt,
            device_id_type=MESH,
        ).wait_send()

    count = [0]

    def local(src, dst):
        copy = pltpu.make_async_copy(src, dst, local_sem.at[count[0]])
        count[0] += 1
        copy.start()
        return copy

    load_qk = [
        local(query_hbm, turn_qk.at[pl.ds(0, DK)]),
        local(key_hbm, turn_qk.at[pl.ds(DK, DK)]),
    ]
    load_vgo = [
        local(value_hbm, w_qo.at[z, x, :, pl.ds(128, 128)]),
        local(gate_hbm, w_qo.at[z, x, :, pl.ds(256, 128)]),
        local(out_w_hbm, w_qo.at[z, x, :, pl.ds(384, 128)]),
    ]
    load_tok = [local(tok_hbm, tok.at[y, c])]
    load_gu = []
    for j in range(6):
        width = 128 if j < 5 else 64
        for k, source in enumerate((ffn_gate_hbm, ffn_up_hbm)):
            place = pl.ds(256 * j + width * k, width)
            load_gu.append(local(source.at[pl.ds(128 * j, width)], turn_gu.at[place]))
    load_down = [local(down_hbm, down_in)]
    load_rest = [
        local(mix_gain_hbm, mix_gain),
        local(ffn_gain_hbm, ffn_gain),
        local(head_gain_hbm, head_gain),
        local(cos_hbm, cos_ref),
        local(sin_hbm, sin_ref),
        local(rate_hbm, rate_ref),
    ]

    def loaded(copies):
        for copy in copies:
            copy.wait()

    loaded(load_qk)
    w_qo[z, x, :, 0:128] = turn_qk[...].T
    loaded(load_vgo)
    loaded(load_tok)
    pl.semaphore_wait(barrier, len(peers))

    def stage_gate_up(_):
        loaded(load_gu)
        for j in range(11):
            lanes = slice(128 * j, 128 * j + 128)
            w_gu[z, x, :, lanes] = turn_gu[lanes, :].T

    def stage_down(_):
        loaded(load_down)
        top, low = down_in[0:352, :], down_in[352:704, :]
        w_d0[z, x] = jnp.concatenate([top[:, :64], low[:, :64]], axis=1)
        w_d1[z, x] = jnp.concatenate([top[:, 64:], low[:, 64:]], axis=1)

    def stage_rest(_):
        loaded(load_rest)
        gap = lax.broadcasted_iota(jnp.int32, (SEQ, 128), 0) - lax.broadcasted_iota(
            jnp.int32, (SEQ, 128), 1
        )
        rate = rate_ref[tp][:1, :]
        for half in range(2):
            distance = (gap - 128 * half).astype(F32)
            mask[:, 128 * half : 128 * half + 128] = jnp.where(
                distance >= 0.0, jnp.exp(jnp.maximum(distance, 0.0) * rate), 0.0
            )

    def rows_of(ch):
        return pl.ds(SEQ * ch, SEQ), pl.ds(SEQ * ch, 128), pl.ds(SEQ * ch + 128, 128)

    def gather_own(buf, tag, ch):
        rows, _, _ = rows_of(ch)
        own = buf.at[y, c, rows]
        send((tag, 0), (tag, 0, ch), own, own, to_yp)
        send((tag, 0), (tag, 1, ch), own, own, to_ym)
        send((tag, 1), (tag, 3, ch), own, own, to_pt)

    def gather_forward(buf, tag, ch, side):
        rows, low, high = rows_of(ch)
        row, part, device = ((ym, low, to_yp), (yp, high, to_ym))[side]
        recv((tag, side, ch), buf.at[row, c, rows])
        send((tag, 0), (tag, 2, ch), buf.at[row, c, part], buf.at[row, c, part], device)
        send((tag, 1), (tag, 3, ch), buf.at[row, c, rows], buf.at[row, c, rows], to_pt)

    def gather_far(buf, tag, ch):
        rows, _, _ = rows_of(ch)
        recv((tag, 2, ch), buf.at[y2, c, rows])
        send((tag, 1), (tag, 3, ch), buf.at[y2, c, rows], buf.at[y2, c, rows], to_pt)

    def gather_done(buf, tag, ch):
        rows, _, _ = rows_of(ch)
        recv((tag, 3, ch), buf.at[:, oc, rows])

    buffers = (w_qo, w_gu, w_gu, w_d0, w_d1)

    def spans(unit):
        first, a, a0, b, b0 = UNITS[unit]
        half_a = (pl.ds(first, a), pl.ds(first, a0), pl.ds(first + a0, a - a0))
        first = first + a
        return half_a, (pl.ds(first, b), pl.ds(first, b0), pl.ds(first + b0, b - b0))

    near = ((xm, xp), (zm, zp))
    far = (x2, z2)
    devices = ((to_xp, to_xm), (to_zp, to_zm))

    def near_at(axis, place):
        return (z, place) if axis == 0 else (place, x)

    def near_own(unit, axis):
        w, name = buffers[unit], WEIGHT_OF[unit]
        half = spans(unit)[axis][0]
        own = w.at[z, x, half]
        for way in range(2):
            send((name, 0), (unit, 0, axis, way), own, own, devices[axis][way])

    def near_forward(unit, axis, way):
        w, name = buffers[unit], WEIGHT_OF[unit]
        at = near_at(axis, near[axis][way])
        half = spans(unit)[axis]
        recv((unit, 0, axis, way), w.at[(*at, half[0])])
        part = w.at[(*at, half[1 + way])]
        send((name, 0), (unit, 1, axis), part, part, devices[axis][way])

    crossed = ((x, xm, xp, x2), (z, zm, zp, z2))

    def far_at(axis, place, i):
        return (place, crossed[0][i]) if axis == 0 else (crossed[1][i], place)

    def far_own(unit, axis, i):
        w, name = buffers[unit], WEIGHT_OF[unit]
        half = spans(unit)[axis][0]
        block = w.at[(*far_at(axis, (z, x)[axis], i), half)]
        if i == 3:
            recv((unit, 1, axis), block)
        for way in range(2):
            send((name, 1), (unit, 2, axis, way, i), block, block, devices[1 - axis][way])

    def far_forward(unit, axis, way, i):
        w, name = buffers[unit], WEIGHT_OF[unit]
        at = far_at(axis, near[1 - axis][way], i)
        half = spans(unit)[axis]
        recv((unit, 2, axis, way, i), w.at[(*at, half[0])])
        part = w.at[(*at, half[1 + way])]
        send((name, 1), (unit, 3), part, part, devices[1 - axis][way])

    def weight_done(unit):
        first, a, _, b, _ = UNITS[unit]
        recv((unit, 3), buffers[unit].at[0, :, pl.ds(first, a + b)])

    mixer_bufs = (part1, pair1, sums1, ends1, relay1)
    ffn_bufs = (
        (part2, pair2, sums2, ends2, relay2),
        (part3, pair3, sums3, ends3, relay3),
    )

    def sum_pair(bufs, tag, ch):
        part, pair = bufs[:2]
        rows, _, _ = rows_of(ch)
        send((tag, 1), (tag, 0, ch), part.at[oc, :, rows], pair.at[:, rows], to_pt)

    def sum_start(bufs, tag, ch):
        part, pair, sums, ends, relay = bufs
        rows, low, high = rows_of(ch)
        half = pl.ds(128 * ch, 128)
        recv((tag, 0, ch), pair.at[:, rows])
        for place in (y2, yp, ym):
            sums[place, rows] = (
                part[c, place, rows].astype(F32) + pair[place, rows].astype(F32)
            ).astype(BF16)
        send((tag, 0), (tag, 1, ch), sums.at[y2, low], relay.at[0, half], to_yp)
        send((tag, 0), (tag, 2, ch), sums.at[y2, high], relay.at[1, half], to_ym)
        send((tag, 0), (tag, 3, ch), sums.at[yp, high], ends.at[1, high], to_yp)
        send((tag, 0), (tag, 3, ch), sums.at[ym, low], ends.at[0, low], to_ym)

    def sum_relay(bufs, tag, ch, side):
        _, _, sums, ends, relay = bufs
        _, low, high = rows_of(ch)
        half = pl.ds(128 * ch, 128)
        place, part, device = ((yp, low, to_yp), (ym, high, to_ym))[side]
        recv((tag, 1 + side, ch), relay.at[side, half])
        sums[place, part] = (
            sums[place, part].astype(F32) + relay[side, half].astype(F32)
        ).astype(BF16)
        send((tag, 0), (tag, 3, ch), sums.at[place, part], ends.at[1 - side, part], device)

    def sum_end(bufs, tag, ch):
        part, pair, _, ends, _ = bufs
        rows, _, _ = rows_of(ch)
        recv((tag, 3, ch), ends.at[:, rows])
        return (part[c, y, rows].astype(F32) + pair[y, rows].astype(F32)) + (
            ends[0, rows].astype(F32) + ends[1, rows].astype(F32)
        )

    def mixer_end(ch):
        rows, _, _ = rows_of(ch)
        total = sum_end(mixer_bufs, 12, ch)
        resid[y, c, rows] = (tok[y, c, rows].astype(F32) + total).astype(BF16)

    def ffn_end(ch, half):
        rows, _, _ = rows_of(ch)
        total = sum_end(ffn_bufs[half], 13 + half, ch)
        if half == 0:
            first[rows] = total
            return
        total = jnp.concatenate(
            [first[rows, :64], total[:, :64], first[rows, 64:], total[:, 64:]], axis=1
        )
        out_ref[rows, :] = (resid[y, c, rows].astype(F32) + total).astype(BF16)

    def norm_rows(buf, gain, ch):
        def body(i, carry):
            rows = pl.ds(pl.multiple_of(SEQ * ch + 32 * i, 32), 32)
            squares = None
            for p in range(8):
                block = buf[p // 2, p % 2, rows].astype(F32)
                squares = block * block if p == 0 else squares + block * block
            mean = jnp.sum(squares, axis=-1, keepdims=True) * (1.0 / 2048.0)
            factor = lax.rsqrt(mean + EPS)
            for p in range(8):
                lanes = slice(256 * p, 256 * p + 256)
                block = buf[p // 2, p % 2, rows].astype(F32)
                normed[rows, lanes] = (block * factor * gain[:, lanes]).astype(BF16)
            return carry

        lax.fori_loop(0, 8, body, 0, unroll=4)

    def mixer(ch):
        rows, _, _ = rows_of(ch)
        qkv = dot(normed[rows, :], w_qo[:, :, :, 0:256].reshape(2048, 256))
        gate = dot(normed[rows, :], w_qo[:, :, :, 256:384].reshape(2048, 128))
        gate = gate.astype(BF16).astype(F32)
        qk = qkv[:, :128].astype(BF16).astype(F32)
        value = qkv[:, 128:].astype(BF16)
        lane = lax.broadcasted_iota(jnp.int32, (SEQ, 128), 1)
        turned = jnp.where(
            lax.rem(lane, 2) == 0, pltpu.roll(qk, 127, axis=1), pltpu.roll(qk, 1, axis=1)
        )
        rotated = qk * cos_ref[...] + turned * sin_ref[...]
        queries = jnp.where(lane < DK, rotated, 0.0).astype(BF16)
        keys = pltpu.roll(rotated, DK, axis=1).astype(BF16)
        scores = lax.dot_general(
            queries, keys, (((1,), (1,)), ((), ())), preferred_element_type=F32
        )
        retained = dot((scores * mask[...]).astype(BF16), value)
        center = jnp.mean(retained, axis=-1, keepdims=True)
        moved = retained - center
        spread = jnp.mean(moved * moved, axis=-1, keepdims=True)
        grouped = moved * lax.rsqrt(spread + EPS) * head_gain[...]
        mixed[rows] = (grouped * silu(gate)).astype(BF16)

    def mixer_out(ch):
        rows, _, _ = rows_of(ch)

        def body(p, carry):
            py, pc = lax.div(p, 2), lax.rem(p, 2)
            block = jnp.concatenate(
                [w_qo[py, 2 * pc, :, 384:512], w_qo[py, 2 * pc + 1, :, 384:512]], axis=1
            )
            part1[pc, py, rows] = dot(mixed[rows], block).astype(BF16)
            return carry

        lax.fori_loop(0, 8, body, 0, unroll=True)

    def gate_up(ch, first):
        rows, _, _ = rows_of(ch)

        def body(j, carry):
            columns = pl.ds(pl.multiple_of(256 * j, 256), 256)
            both = dot(normed[rows, :], w_gu[:, :, :, columns].reshape(2048, 256))
            hidden[rows, pl.ds(pl.multiple_of(128 * j, 128), 128)] = (
                silu(both[:, :128]) * both[:, 128:]
            ).astype(BF16)
            return carry

        if first:
            lax.fori_loop(0, 3, body, 0, unroll=True)
            return
        lax.fori_loop(3, 5, body, 0, unroll=True)
        both = dot(normed[rows, :], w_gu[:, :, :, 1280:1408].reshape(2048, 128))
        hidden[rows, 640:768] = (silu(both) * pltpu.roll(both, 64, axis=1)).astype(BF16)

    def join(half):
        w = (w_d0, w_d1)[half]
        for py in range(4):
            top, low = [], []
            for k in range(4):
                block = w[py, k]
                top.append(block[:, :64])
                low.append(block[:, 64:])
            joined[half, py, 0:352, :] = jnp.concatenate(top, axis=1)
            joined[half, py, 352:704, :] = jnp.concatenate(low, axis=1)

    def down(ch, half):
        rows, _, _ = rows_of(ch)
        target = (part2, part3)[half]
        for py in range(4):
            both = dot(hidden[rows, :704], joined[half, py]).astype(BF16)
            target[0, py, rows] = both[:, :128]
            target[1, py, rows] = both[:, 128:]

    part = functools.partial
    actions = [part(near_own, axis=axis) for axis in range(2)]
    actions += [part(near_forward, axis=k // 2, way=k % 2) for k in range(4)]
    actions += [part(far_own, axis=k // 4, i=k % 4) for k in range(8)]
    actions += [part(far_forward, axis=k // 8, way=k // 4 % 2, i=k % 4) for k in range(16)]
    actions += [weight_done, stage_gate_up, stage_down, stage_rest]
    for tag, buf in ((10, tok), (11, resid)):
        actions.append(part(gather_own, buf, tag))
        actions += [part(gather_forward, buf, tag, side=side) for side in range(2)]
        actions += [part(gather_far, buf, tag), part(gather_done, buf, tag)]
    for tag, bufs, end in (
        (12, mixer_bufs, mixer_end),
        (13, ffn_bufs[0], part(ffn_end, half=0)),
        (14, ffn_bufs[1], part(ffn_end, half=1)),
    ):
        actions += [part(sum_pair, bufs, tag), part(sum_start, bufs, tag)]
        actions += [part(sum_relay, bufs, tag, side=side) for side in range(2)]
        actions.append(end)
    actions += [part(norm_rows, tok, mix_gain), mixer, mixer_out]
    actions += [part(norm_rows, resid, ffn_gain)]
    actions += [part(gate_up, first=True), part(gate_up, first=False)]
    actions += [part(down, half=0), part(down, half=1), join]
    for code in SCHEDULE:
        actions[code // 8](code % 8)

    for name, w in enumerate((w_qo, w_gu, w_d0, w_d1)):
        all_sent((name, 0), w.at[0, pl.ds(0, 3)])
        all_sent((name, 1), w.at[pl.ds(0, 3)])
    for tag, buf in ((10, tok), (11, resid)):
        all_sent((tag, 0), buf.at[pl.ds(0, 3), 0])
        all_sent((tag, 1), buf.at[:, 0])
    for tag, bufs in ((12, mixer_bufs), (13, ffn_bufs[0]), (14, ffn_bufs[1])):
        all_sent((tag, 0), bufs[2].at[pl.ds(0, 3)])
        all_sent((tag, 1), bufs[0].at[0])
    assert len(ids) == RECEIVES and len(groups) == SENDS


def per_device(*args):
    (tokens, mix_gain, query_w, key_w, value_w, gate_w, out_w, head_gain, ffn_gain) = args[:9]
    ffn_gate, ffn_up, ffn_down = args[9:]
    cosine, sine = rope_tables()
    hbm = pl.BlockSpec(memory_space=pltpu.HBM)
    rows = tokens.shape[0]

    def sum_buffers(width):
        return [
            pltpu.VMEM((2, 4, rows, width), BF16),
            pltpu.VMEM((4, rows, width), BF16),
            pltpu.VMEM((4, rows, width), BF16),
            pltpu.VMEM((2, rows, width), BF16),
            pltpu.VMEM((2, rows // 2, width), BF16),
        ]

    call = pl.pallas_call(
        layer_kernel,
        out_shape=pltpu.VMEM((rows, 256), BF16),
        in_specs=[hbm] * 15,
        out_specs=pl.BlockSpec(memory_space=pltpu.VMEM),
        scratch_shapes=[
            pltpu.VMEM((4, 2, rows, 256), BF16),
            pltpu.VMEM((4, 2, rows, 256), BF16),
            pltpu.VMEM((rows, 2048), BF16),
            pltpu.VMEM((4, 4, 128, 512), BF16),
            pltpu.VMEM((4, 4, 128, 1408), BF16),
            pltpu.VMEM((4, 4, 352, 128), BF16),
            pltpu.VMEM((4, 4, 352, 128), BF16),
            pltpu.VMEM((2, 4, 704, 256), BF16),
            pltpu.VMEM((704, 128), BF16),
            pltpu.VMEM((2 * DK, 128), BF16),
            pltpu.VMEM((1408, 128), BF16),
            pltpu.VMEM((1, 2048), F32),
            pltpu.VMEM((1, 2048), F32),
            pltpu.VMEM((1, DV), F32),
            pltpu.VMEM((SEQ, 128), F32),
            pltpu.VMEM((SEQ, 128), F32),
            pltpu.VMEM((HEADS, 8, 128), F32),
            pltpu.VMEM((SEQ, SEQ), F32),
            pltpu.VMEM((rows, DV), BF16),
            pltpu.VMEM((rows, 768), BF16),
            *sum_buffers(256),
            *sum_buffers(128),
            *sum_buffers(128),
            pltpu.VMEM((rows, 128), F32),
            pltpu.SemaphoreType.DMA((32,)),
            pltpu.SemaphoreType.DMA((SENDS,)),
            pltpu.SemaphoreType.DMA((RECEIVES,)),
        ],
        compiler_params=pltpu.CompilerParams(
            collective_id=0, has_side_effects=True, vmem_limit_bytes=54 * 2**20
        ),
        cost_estimate=pl.CostEstimate(
            flops=11_000_000_000, bytes_accessed=4_000_000, transcendentals=1_000_000
        ),
        name="layer",
    )
    return call(
        tokens,
        mix_gain.reshape(1, -1),
        query_w.T,
        key_w.T,
        value_w,
        gate_w,
        out_w,
        head_gain,
        ffn_gain.reshape(1, -1),
        ffn_gate.T,
        ffn_up.T,
        ffn_down,
        jnp.asarray(cosine),
        jnp.asarray(sine),
        jnp.asarray(decay_table()),
    )


def solution(mesh):
    placed = (
        P(("rep", "fs"), "tp"),
        P(),
        P("fs", "tp"),
        P("fs", "tp"),
        P("fs", "tp"),
        P("fs", "tp"),
        P("tp", "fs"),
        P("tp", None),
        P(),
        P("fs", "tp"),
        P("fs", "tp"),
        P("tp", "fs"),
    )
    return jax.shard_map(
        per_device, mesh=mesh, in_specs=placed, out_specs=P(("rep", "fs"), "tp"), check_vma=False
    )
```
